32 devices in a mesh: ep: 8 (over z, x), tp: 4 (over y, core).
Axes of the slice: x: 2, y: 2, z: 4, core: 2. Of those that a mesh axis runs over, the one named last changes fastest.
Arguments:
- filter_value: bfloat16 [8192, 1024], P(('ep', 'tp')), may hold values from -6 to 6
- filter_gate: bfloat16 [8192, 1024], P(('ep', 'tp')), may hold values from -9 to 9
- filter_taps: float32 [31, 1024], replicated, may hold values from -1 to 1
- filter_bias: float32 [1024], replicated, may hold values from -3 to 3
- norm_gain: float32 [1024], replicated, may hold values from 0.1 to 1.9
- norm_shift: float32 [1024], replicated, may hold values from -3 to 3
- out_weight: bfloat16 [1024, 2048], replicated, may hold values from -0.1875 to 0.1875
- out_bias: float32 [2048], replicated, may hold values from -3 to 3
- expert_input: bfloat16 [2048, 2048], P('ep'), may hold values from -6 to 6
- expert_gain: float32 [2048], replicated, may hold values from 0.1 to 1.9
- route_experts: int32 [2048, 2], P('ep'), may hold values from 0 to 7, all different within a row; in each aligned block of 256 rows (0 to 255, 256 to 511, ...) at most 128 rows name the same one
- route_weights: float32 [2048, 2], P('ep'), may hold values from 0.2 to 1
- gate_weights: bfloat16 [8, 2048, 2048], P('ep', None, 'tp'), may hold values from -0.375 to 0.375
- up_weights: bfloat16 [8, 2048, 2048], P('ep', None, 'tp'), may hold values from -0.375 to 0.375
- down_weights: bfloat16 [8, 2048, 2048], P('ep', 'tp'), may hold values from -0.0234375 to 0.0234375
Outputs:
- mixer_out: bfloat16 [8192, 2048], P(('ep', 'tp'))
- expert_out: bfloat16 [2048, 2048], P('ep', 'tp')
The draws below stay inside these ranges and needn't reach their ends.
Inputs may be any that keep to these rules, and one draw needn't show every extreme that they name: `route_experts`: each row names 2 different experts. Within the rows of one index of ep (aligned blocks of 256 rows) no expert is named by more than 128 rows, a bound that some block reaches.
All inputs are finite; a program needn't handle non-finite values.
Results may differ from the reference program's by a relative error of at most 0.012.
Values may be sent and summed in bfloat16 or wider, within the bound.
A program may use at most 128 MiB of HBM per device.

```python
import math
import jax
import jax.numpy as jnp
import numpy as np
from jax import lax

D = 2048
CHANNELS = 1024
TAPS = 31
HIDDEN_SIZE = 2048
TOPK = 2
ROUTE_DEV = 256
EXPERTS = 8
CAPACITY = 128
MIX_TOKENS = 8192
ROUTE_TOKENS = 2048
N_EP = 8
N_TP = 4


def level_of(rng, shape, split, low, top_value):
    def one(axis_at, parts):
        draws = jax.random.uniform(jax.random.fold_in(jax.random.fold_in(rng, 6), axis_at), (parts,), jnp.float32, low / len(split), top_value / len(split))
        return jnp.repeat(jnp.exp(draws), shape[axis_at] // parts).reshape((-1,) + (1,) * (len(shape) - axis_at - 1))

    factor_of = one(*split[0])
    for cut in split[1:]:
        factor_of = factor_of * one(*cut)
    return factor_of


def deal_out(stream_key, own, number, rows, count, top, reach, lean):
    sequence = jax.random.permutation(stream_key, count)
    heavy_load, ordinary = shares(count, rows * top, reach, lean, True), shares(count, rows * top, reach, lean, False)
    places = jnp.arange(count)

    def named(tallies, turn):
        used = int((tallies > 0).sum())
        fixed = max(1, used // 4)
        passed = fixed + (places - fixed + turn * (used - fixed)) % max(1, count - fixed)
        return jnp.zeros((count,), jnp.int32).at[sequence[jnp.where(places < fixed, places, passed)]].set(jnp.asarray(tallies, jnp.int32))

    tallies = jnp.where(number % 4 == 0, named(heavy_load, number // 4), named(ordinary, number - number // 4 - 1))
    mixed = jax.random.permutation(jax.random.fold_in(own, 3), count)
    giver, taker = mixed[0:count // 2 * 2:2], mixed[1:count // 2 * 2:2]
    margin = jnp.minimum(tallies[giver] - 1, reach - tallies[taker]) // 2
    margin = jnp.where((giver == sequence[0]) | (taker == sequence[0]) | (tallies[taker] == 0), 0, jnp.maximum(margin, 0))
    passed = jax.random.randint(jax.random.fold_in(own, 4), (count // 2,), 0, 1 << 20) % (margin + 1)
    tallies = tallies.at[giver].add(-passed).at[taker].add(passed)
    items = jnp.searchsorted(jnp.cumsum(tallies), jnp.arange(rows * top), side="right").astype(jnp.int32)
    grid = items.reshape(top, rows).T
    grid = grid[jax.random.permutation(jax.random.fold_in(own, 1), rows)]
    turn = jax.random.randint(jax.random.fold_in(own, 2), (rows, 1), 0, top)
    return jnp.take_along_axis(grid, (jnp.arange(top)[None, :] + turn) % top, axis=1)


def shares(number_of, total, bound, slope, full):
    loads = [(1 << 20) // math.isqrt(grade ** slope) + 1 for grade in range(1, number_of + 1)]
    largest = bound if full else min(bound, max(-(-total // number_of), total * loads[0] // sum(loads)))
    least = 1 if total - largest >= number_of - 1 else 0
    given, spare = [largest] + [least] * (number_of - 1), total - largest - least * (number_of - 1)
    while spare > 0:
        movable = [i for i in range(1, number_of) if given[i] < largest] or [i for i in range(1, number_of) if given[i] < bound]
        whole, budget = sum([loads[i] for i in movable]), spare
        for i in movable:
            extra = min(bound - given[i], max(1, budget * loads[i] // whole), spare)
            given[i] = given[i] + extra
            spare = spare - extra
    return np.array(given)


def bell_draw(key, extent, width, reach, split=(), held_as=jnp.bfloat16):
    values = width * jax.random.normal(key, extent, jnp.float32)
    if split:
        values = values * level_of(key, extent, split, -0.22, 0.18)
    return jnp.clip(values, -reach, reach).astype(held_as)


def setup_inputs(seed: int = 0) -> dict:
    key_of = jax.random.split(jax.random.key(seed), 16)
    filter_value = bell_draw(key_of[0], (MIX_TOKENS, CHANNELS), 1.0, 6.0, ((0, 32),))
    filter_gate = bell_draw(key_of[1], (MIX_TOKENS, CHANNELS), 1.5, 9.0, ((0, 32),))
    filter_taps = bell_draw(key_of[2], (TAPS, CHANNELS), TAPS ** -0.5, 1.0, (), jnp.float32)
    filter_bias = bell_draw(key_of[3], (CHANNELS,), 0.5, 3.0, (), jnp.float32)
    norm_gain = jnp.clip(1.0 + 0.18 * jax.random.normal(key_of[4], (CHANNELS,), jnp.float32), 0.1, 1.9)
    norm_shift = bell_draw(key_of[5], (CHANNELS,), 0.5, 3.0, (), jnp.float32)
    out_weight = bell_draw(key_of[6], (CHANNELS, D), CHANNELS ** -0.5, 0.1875)
    out_bias = bell_draw(key_of[7], (D,), 0.5, 3.0, (), jnp.float32)
    expert_input = bell_draw(key_of[8], (ROUTE_TOKENS, D), 1.0, 6.0, ((0, 8),))
    expert_gain = jnp.clip(1.0 + 0.18 * jax.random.normal(key_of[9], (D,), jnp.float32), 0.1, 1.9)
    route_experts_keys = jax.random.split(jax.random.fold_in(key_of[10], 1), ROUTE_TOKENS // ROUTE_DEV)
    route_experts_turns = jax.random.permutation(jax.random.fold_in(key_of[10], 3), ROUTE_TOKENS // ROUTE_DEV)
    route_experts = jax.vmap(lambda own, number: deal_out(jax.random.fold_in(key_of[10], 2), own, number, ROUTE_DEV, EXPERTS, TOPK, CAPACITY, 2))(route_experts_keys, route_experts_turns).reshape((ROUTE_TOKENS, TOPK))
    route_weights = jnp.clip(0.2 + 0.8 * jax.random.uniform(key_of[11], (ROUTE_TOKENS, TOPK), jnp.float32) ** level_of(key_of[11], (ROUTE_TOKENS, TOPK), ((0, 8),), -0.2, 0.2), 0.2, 1.0)
    gate_weights = bell_draw(key_of[12], (EXPERTS, D, HIDDEN_SIZE), (D // 8) ** -0.5, 0.375, ((0, 8), (2, 4)))
    up_weights = bell_draw(key_of[13], (EXPERTS, D, HIDDEN_SIZE), (D // 8) ** -0.5, 0.375, ((0, 8), (2, 4)))
    down_weights = bell_draw(key_of[14], (EXPERTS, HIDDEN_SIZE, D), (36 * HIDDEN_SIZE) ** -0.5, 0.0234375, ((0, 8), (1, 4)))
    return dict(filter_value=filter_value, filter_gate=filter_gate, filter_taps=filter_taps, filter_bias=filter_bias, norm_gain=norm_gain, norm_shift=norm_shift, out_weight=out_weight, out_bias=out_bias, expert_input=expert_input, expert_gain=expert_gain, route_experts=route_experts, route_weights=route_weights, gate_weights=gate_weights, up_weights=up_weights, down_weights=down_weights)


epsilon = 1e-06
clamp_limit = 7.0
swish_alpha = 1.702

def reference(filter_value, filter_gate, filter_taps, filter_bias, norm_gain, norm_shift, out_weight, out_bias, expert_input, expert_gain, route_experts, route_weights, gate_weights, up_weights, down_weights):
    gated = (filter_value.astype(jnp.float32) * jax.nn.sigmoid(filter_gate.astype(jnp.float32))).astype(jnp.bfloat16)
    length = gated.shape[0]
    padded = jnp.concatenate([jnp.zeros((TAPS - 1, CHANNELS), jnp.bfloat16), gated], 0)
    filtered = jnp.zeros((length, CHANNELS), jnp.float32)
    for offset in range(TAPS):
        filtered = filtered + filter_taps[offset] * padded[offset:offset + length].astype(jnp.float32)
    filtered = filtered + filter_bias
    average = lax.optimization_barrier(jnp.mean(filtered, 1, keepdims=True))
    centred = filtered - average
    variance = lax.optimization_barrier(jnp.mean(centred * centred, 1, keepdims=True))
    normed_filter = centred * lax.rsqrt(variance + epsilon) * norm_gain + norm_shift
    activated = jax.nn.silu(normed_filter).astype(jnp.bfloat16)
    mixer_out = (jnp.dot(activated, out_weight, preferred_element_type=jnp.float32) + out_bias).astype(jnp.bfloat16)
    token_values = expert_input.astype(jnp.float32)
    normed = (token_values * lax.rsqrt(lax.optimization_barrier(jnp.mean(token_values * token_values, 1, keepdims=True)) + epsilon) * expert_gain).astype(jnp.bfloat16)
    blocked = route_experts.reshape(N_EP, ROUTE_DEV * TOPK)
    onehot = (blocked[:, :, None] == jnp.arange(EXPERTS, dtype=jnp.int32)[None, None, :]).astype(jnp.int32)
    earlier = jnp.cumsum(onehot, 1) - onehot
    slot = lax.optimization_barrier(jnp.sum(earlier * onehot, 2)).astype(jnp.int32)
    row_slot = (jnp.arange(N_EP, dtype=jnp.int32)[:, None] * CAPACITY + slot).reshape(-1).astype(jnp.int32)
    flat_ids = route_experts.reshape(-1).astype(jnp.int32)
    copies = jnp.repeat(normed, TOPK, axis=0)
    buffer = jnp.zeros((EXPERTS, N_EP * CAPACITY, D), jnp.bfloat16).at[flat_ids, row_slot].set(copies)

    def expert_rows(operands):
        rows_in, gate_matrix, up_matrix, down_matrix = operands
        gate_pre = jnp.dot(rows_in, gate_matrix, preferred_element_type=jnp.float32)
        up_pre = jnp.dot(rows_in, up_matrix, preferred_element_type=jnp.float32)
        gate_held = jnp.minimum(gate_pre, clamp_limit)
        up_held = jnp.clip(up_pre, -clamp_limit, clamp_limit)
        hidden = (gate_held * jax.nn.sigmoid(swish_alpha * gate_held) * (up_held + 1.0)).astype(jnp.bfloat16)
        shards = hidden.reshape(-1, N_TP, HIDDEN_SIZE // N_TP).astype(jnp.float32)
        down_shards = down_matrix.reshape(N_TP, HIDDEN_SIZE // N_TP, D).astype(jnp.float32)
        partial_value = jnp.einsum('rpf,pfd->prd', shards, down_shards).astype(jnp.bfloat16)
        partial_value = lax.optimization_barrier(partial_value)
        return lax.optimization_barrier(jnp.sum(partial_value.astype(jnp.float32), 0)).astype(jnp.bfloat16)
    results = lax.map(expert_rows, (buffer, gate_weights, up_weights, down_weights))
    picked = results[flat_ids, row_slot].astype(jnp.float32).reshape(-1, TOPK, D)
    expert_out = lax.optimization_barrier(jnp.sum(picked * route_weights[:, :, None], 1)).astype(jnp.bfloat16)
    return (mixer_out, expert_out)
```

```python
import functools

import jax
import jax.numpy as jnp
from jax import lax
from jax.experimental import pallas as pl
from jax.experimental.pallas import tpu as pltpu
from jax.sharding import PartitionSpec as P

epsilon = 1e-06
clamp_limit = 7.0
swish_alpha = 1.702
LANES = 128
SCHEDULE = (
    "C0 F0 D0 S1",
    "F1 F2 F3 A1",
    "A2 S2 C1 F4",
    "D1 E0 B2 F5",
    "A4 C2 S3 A3",
    "F6 D2 C3 B4",
    "E1 D3 C4 A6",
    "E2 D4 A7 A5",
    "C5 B6 F7 C6",
    "E4 D6 B7 E3",
    "C7 E6 D7 D5",
    "E7 E5",
)
f32 = jnp.float32
bf16 = jnp.bfloat16


def dot(a, b):
    return jnp.dot(a, b, preferred_element_type=f32)


def kernel(
    n_ep,
    n_tp,
    capacity,
    value_hbm,
    gate_hbm,
    taps_hbm,
    bias_hbm,
    gain_hbm,
    shift_hbm,
    out_weight_hbm,
    out_bias_hbm,
    tokens_hbm,
    expert_gain_hbm,
    route_t_hbm,
    route_weight_t_hbm,
    gate_w_hbm,
    up_w_hbm,
    down_w_hbm,
    mixer,
    expert_out_ref,
    value,
    gate,
    taps_ref,
    bias_ref,
    gain_ref,
    shift_ref,
    out_weight,
    out_bias_ref,
    tokens_ref,
    expert_gain_ref,
    route_t_ref,
    route_weight_t_ref,
    gate_w,
    up_w,
    down_w,
    halo_out,
    halo_in,
    padded,
    filtered,
    activated,
    outgoing,
    outgoing_wide,
    arrived,
    hidden,
    partial,
    half_in,
    pair_out,
    pair_in,
    summed,
    returned,
    weight_high,
    weight_low,
    load_sem,
    halo_sem,
    disp_send,
    disp_recv,
    wide_send,
    wide_recv,
    f1_send,
    f1_recv,
    f2_send,
    f2_recv,
    r1_send,
    r1_recv,
    r2_send,
    r2_recv,
    ret_send,
    ret_recv,
):
    i = lax.axis_index("ep")
    q = lax.axis_index("tp")
    q1 = q + 1 - 2 * lax.rem(q, 2)
    q2 = lax.rem(q + 2, 4)
    q3 = lax.rem(q1 + 2, 4)
    tokens, width = tokens_ref.shape
    cols = width // n_tp
    rows_all = n_ep * capacity
    group_rows = max(128, capacity)
    per_group = group_rows // capacity
    groups = rows_all // group_rows
    length, channels = value.shape
    lane_tiles = channels // LANES
    taps = taps_ref.shape[0]
    rim = halo_out.shape[0]
    single = per_group == 1
    near = n_ep // 2 if single else 0
    here = i * n_tp + q
    last = n_ep * n_tp - 1
    following = lax.rem(here + 1, n_ep * n_tp)

    def peer(k):
        other, bit = 0, 1
        while bit < n_ep:
            other = other + bit * lax.rem(i // bit + k // bit, 2)
            bit *= 2
        return other

    barrier = pltpu.get_barrier_semaphore()

    def greet(ep, tp):
        pl.semaphore_signal(
            barrier,
            inc=1,
            device_id={"ep": ep, "tp": tp},
            device_id_type=pl.DeviceIdType.MESH,
        )

    def greet_peer(k, c):
        greet(peer(k), q)
        return c

    lax.fori_loop(1, n_ep, greet_peer, 0)
    greet(i, q1)
    greet(i, q2)

    @pl.when(here > 0)
    def _():
        greet((here - 1) // n_tp, lax.rem(here - 1, n_tp))

    copies = (
        ("route", route_t_hbm, route_t_ref),
        ("tokens", tokens_hbm, tokens_ref),
        ("expert_gain", expert_gain_hbm, expert_gain_ref),
        ("value", value_hbm, value),
        ("gate", gate_hbm, gate),
        ("taps", taps_hbm, taps_ref),
        ("bias", bias_hbm, bias_ref),
        ("gain", gain_hbm, gain_ref),
        ("shift", shift_hbm, shift_ref),
        ("out_bias", out_bias_hbm, out_bias_ref),
        ("weight_t", route_weight_t_hbm, route_weight_t_ref),
        ("gate_w", gate_w_hbm.at[0], gate_w),
        ("up_w", up_w_hbm.at[0], up_w),
        ("down_w", down_w_hbm.at[0], down_w),
        ("out_weight", out_weight_hbm, out_weight),
    )
    names = [name for name, _, _ in copies]
    loads = {
        name: pltpu.make_async_copy(s, d, load_sem.at[n])
        for n, (name, s, d) in enumerate(copies)
    }
    for name in names[:11]:
        loads[name].start()

    def remote(src, dst, send, recv, ep, tp):
        return pltpu.make_async_remote_copy(
            src_ref=src,
            dst_ref=dst,
            send_sem=send,
            recv_sem=recv,
            device_id={"ep": ep, "tp": tp},
            device_id_type=pl.DeviceIdType.MESH,
        )

    def block(k):
        return pl.ds(pl.multiple_of(k * capacity, capacity), capacity)

    def group(g):
        return pl.ds(pl.multiple_of(g * group_rows, group_rows), group_rows)

    def dispatch(k):
        return remote(
            outgoing.at[block(k)],
            arrived.at[q, block(k)],
            disp_send.at[k],
            disp_recv.at[k],
            peer(k),
            q,
        )

    def dispatch_wide(k):
        return remote(
            outgoing_wide.at[block(k)],
            arrived.at[q2, block(k)],
            wide_send.at[k],
            wide_recv.at[k],
            peer(k),
            q,
        )

    def spread_pair(g):
        at = arrived.at[q, group(g)]
        return remote(at, at, f1_send.at[g], f1_recv.at[g], i, q2)

    def spread_core(g, n):
        at = arrived.at[q if n == 0 else q2, group(g)]
        return remote(at, at, f2_send.at[g, n], f2_recv.at[g, n], i, q1)

    def reduce_core(g, n):
        return remote(
            partial.at[q1 if n == 0 else q3, group(g)],
            half_in.at[n, group(g)],
            r1_send.at[g, n],
            r1_recv.at[g, n],
            i,
            q1,
        )

    def reduce_pair(g):
        return remote(
            pair_out.at[group(g)], pair_in.at[group(g)], r2_send.at[g], r2_recv.at[g], i, q2
        )

    def give_back(k):
        return remote(
            summed.at[block(k)],
            returned.at[block(k)],
            ret_send.at[k],
            ret_recv.at[k],
            peer(k),
            q,
        )

    halo = remote(
        halo_out, halo_in, halo_sem.at[0], halo_sem.at[1], following // n_tp, lax.rem(following, n_tp)
    )

    def lower(a, b):
        return jnp.where(a < b, 1.0, 0.0).astype(bf16)

    side = (tokens, tokens)
    row_id = lax.broadcasted_iota(jnp.int32, side, 0)
    col_id = lax.broadcasted_iota(jnp.int32, side, 1)
    experts_t = lax.broadcasted_iota(jnp.int32, (n_ep, tokens), 0)
    loads["route"].wait()
    picks_t = [route_t_ref[n : n + 1, :] for n in range(route_t_ref.shape[0])]
    hot_t = [jnp.where(experts_t == p, 1.0, 0.0) for p in picks_t]
    rank_t = dot(sum(hot_t).astype(bf16), lower(row_id, col_id))
    slot_rows = lax.broadcasted_iota(jnp.int32, (rows_all, tokens), 0).astype(f32)
    chosen = jnp.zeros((rows_all, tokens), f32)
    targets = []
    for p, h in zip(picks_t, hot_t):
        target = (jnp.bitwise_xor(p, i) * capacity).astype(f32) + jnp.sum(
            rank_t * h, 0, keepdims=True
        )
        targets.append(target)
        chosen = jnp.where(slot_rows == target, 1.0, chosen)

    with jax.named_scope("w_tok"):
        loads["tokens"].wait()
    for name in names[11:]:
        loads[name].start()
    x = tokens_ref[...].astype(f32)
    scale = lax.rsqrt(jnp.mean(x * x, 1, keepdims=True) + epsilon)
    chosen = chosen.astype(bf16)
    loads["expert_gain"].wait()

    def columns(n):
        at = pl.ds(pl.multiple_of(n * cols, cols), cols)
        return (tokens_ref[:, at].astype(f32) * scale * expert_gain_ref[:, at]).astype(bf16)

    with jax.named_scope("select"):
        outgoing[...] = dot(chosen, columns(q)).astype(bf16)
        if near:
            outgoing_wide[...] = dot(chosen[0 : near * capacity], columns(q2)).astype(bf16)
    loads["value"].wait()
    loads["gate"].wait()
    edge = pl.ds(length - rim, rim)
    halo_out[...] = (value[edge].astype(f32) * jax.nn.sigmoid(gate[edge].astype(f32))).astype(bf16)

    with jax.named_scope("w_barrier"):
        pl.semaphore_wait(barrier, n_ep + 2 - jnp.where(here == last, 1, 0))

    @pl.when(here < last)
    def _():
        halo.start()

    @pl.when(here == 0)
    def _():
        halo_in[...] = jnp.zeros_like(halo_in)

    if single and n_ep == 8:
        staged = ((1, -1, 4, 2), (5, -2), (6, 3), (7, -3))
    else:
        staged = (range(1, n_ep),)

    def send(n):
        for k in staged[n] if n < len(staged) else ():
            (dispatch(k) if k > 0 else dispatch_wide(-k)).start()

    with jax.named_scope("wide"):
        send(0)
        if single:
            for n in range(n_tp):
                arrived[n, 0:capacity] = dot(chosen[0:capacity], columns(n)).astype(bf16)
        else:
            arrived[q, 0:capacity] = outgoing[0:capacity]

    def gate_tile(l, c):
        at = pl.ds(pl.multiple_of(l * LANES, LANES), LANES)
        padded[l, rim:] = (
            (value[:, at].astype(f32) * jax.nn.sigmoid(gate[:, at].astype(f32)))
            .astype(bf16)
            .astype(f32)
        )
        return c

    def conv_tile(l, c):
        at = pl.ds(pl.multiple_of(l * LANES, LANES), LANES)
        padded[l, 0:rim] = halo_in[:, at].astype(f32)
        total = jnp.zeros((length, LANES), f32) + bias_ref[:, at]
        for j in range(taps):
            total = total + taps_ref[j : j + 1, at] * padded[l, pl.ds(rim - taps + 1 + j, length)]
        filtered[:, at] = total
        return c

    def norm_rows(r, c):
        at = pl.ds(pl.multiple_of(r * 32, 32), 32)
        f = filtered[at]
        centred = f - jnp.mean(f, 1, keepdims=True)
        variance = jnp.mean(centred * centred, 1, keepdims=True)
        v = centred * lax.rsqrt(variance + epsilon) * gain_ref[...] + shift_ref[...]
        activated[at] = (v * jax.nn.sigmoid(v)).astype(bf16)
        return c

    def project(n, c):
        at = pl.ds(pl.multiple_of(n * 256, 256), 256)
        mixer[:, at] = (dot(activated[...], out_weight[:, at]) + out_bias_ref[:, at]).astype(bf16)
        return c

    def experts_of(gs):
        ats = [group(g) for g in gs]
        held_rows = pl.ds(0, len(gs) * group_rows)

        def unit(n, c):
            u_at = pl.ds(pl.multiple_of(n * 256, 256), 256)
            rows = jnp.concatenate(
                [jnp.concatenate([arrived[s, at] for s in range(n_tp)], 1) for at in ats], 0
            )
            g_pre = dot(rows, gate_w[:, u_at])
            u_pre = dot(rows, up_w[:, u_at])
            held = jnp.minimum(g_pre, clamp_limit)
            up = jnp.clip(u_pre, -clamp_limit, clamp_limit)
            hidden[held_rows, u_at] = (held * jax.nn.sigmoid(swish_alpha * held) * (up + 1.0)).astype(bf16)
            return c

        lax.fori_loop(0, gate_w.shape[1] // 256, unit, 0)

        def down(s, c):
            at_cols = pl.ds(pl.multiple_of(s * cols, cols), cols)
            part = dot(hidden[held_rows, :], down_w[:, at_cols]).astype(bf16)
            for n, at in enumerate(ats):
                partial[s, at] = part[n * group_rows : (n + 1) * group_rows]
            return c

        lax.fori_loop(0, n_tp, down, 0)

    def arrive(k, c):
        dispatch(k).wait_recv()
        return c

    def give(k, c):
        give_back(k).start()
        return c

    if single and n_ep == 8:
        order = [0, 1, 4, 2, 5, 3, 6, 7]
    else:
        order = list(range(groups))
    wide = [g < near for g in order]
    order = [jnp.int32(g) for g in order]

    def take(s):
        g = order[s]
        if single and s == 0:
            return
        with jax.named_scope(f"A{s}"):
            lax.fori_loop(jnp.maximum(g * per_group, 1), (g + 1) * per_group, arrive, 0)
            if wide[s]:
                dispatch_wide(g).wait_recv()
            else:
                spread_pair(g).start()
            spread_core(g, 0).start()
            if wide[s]:
                spread_core(g, 1).start()

    def relay(s):
        g = order[s]
        if wide[s]:
            return
        with jax.named_scope(f"B{s}"):
            spread_pair(g).wait_recv()
            spread_core(g, 1).start()

    def compute(*steps):
        for s in steps:
            if not (single and s == 0):
                with jax.named_scope(f"Cw{s}"):
                    spread_core(order[s], 0).wait_recv()
                    spread_core(order[s], 1).wait_recv()
        with jax.named_scope(f"C{steps}"):
            experts_of([order[s] for s in steps])
        for s in steps:
            reduce_core(order[s], 0).start()
            reduce_core(order[s], 1).start()

    def halve(s):
        g = order[s]
        at = group(g)
        with jax.named_scope(f"D{s}"):
            reduce_core(g, 0).wait_recv()
            reduce_core(g, 1).wait_recv()
            pair_out[at] = (partial[q2, at].astype(f32) + half_in[1, at].astype(f32)).astype(bf16)
            reduce_pair(g).start()

    def finish(s):
        g = order[s]
        at = group(g)
        with jax.named_scope(f"E{s}"):
            reduce_pair(g).wait_recv()
            summed[at] = (
                partial[q, at].astype(f32) + half_in[0, at].astype(f32) + pair_in[at].astype(f32)
            ).astype(bf16)
            lax.fori_loop(jnp.maximum(g * per_group, 1), (g + 1) * per_group, give, 0)

    def mixer_gate():
        lax.fori_loop(0, lane_tiles, gate_tile, 0)

    def mixer_halo():
        for name in ("taps", "bias", "gain", "shift"):
            loads[name].wait()

        @pl.when(here > 0)
        def _():
            halo.wait_recv()

    def mixer_conv(n):
        lax.fori_loop(n * lane_tiles // 2, (n + 1) * lane_tiles // 2, conv_tile, 0)

    def mixer_norm():
        lax.fori_loop(0, length // 32, norm_rows, 0)

    def mixer_project(n):
        if n == 0:
            loads["out_weight"].wait()
            loads["out_bias"].wait()
        tiles = out_weight.shape[1] // 256
        lax.fori_loop(n * tiles // 2, (n + 1) * tiles // 2, project, 0)

    def weigh():
        loads["weight_t"].wait()
        weights = jnp.zeros((rows_all, tokens), f32)
        for n, target in enumerate(targets):
            weights = jnp.where(slot_rows == target, route_weight_t_ref[n : n + 1, :], weights)
        weights = weights.T
        high = weights.astype(bf16)
        weight_high[...] = high
        weight_low[...] = (weights - high.astype(f32)).astype(bf16)

    fillers = [
        mixer_gate,
        mixer_halo,
        functools.partial(mixer_conv, 0),
        functools.partial(mixer_conv, 1),
        mixer_norm,
        functools.partial(mixer_project, 0),
        functools.partial(mixer_project, 1),
        weigh,
    ]

    def fill(n):
        with jax.named_scope(f"F{n}"):
            fillers[n]()

    for name in ("gate_w", "up_w", "down_w"):
        loads[name].wait()
    stages = {"A": take, "B": relay, "S": send, "C": compute, "D": halve, "E": finish, "F": fill}
    for word in " ".join(SCHEDULE).split():
        stages[word[0]](*[int(n) for n in word[1:].split("+")])
    returned[0:capacity] = summed[0:capacity]

    def came_back(k, c):
        give_back(k).wait_recv()
        return c

    with jax.named_scope("w_ret"):
        lax.fori_loop(1, n_ep, came_back, 0)
    with jax.named_scope("final"):
        expert_out_ref[...] = (
            dot(weight_high[...], returned[...]) + dot(weight_low[...], returned[...])
        ).astype(bf16)

    @pl.when(here < last)
    def _():
        halo.wait_send()

    def sent(k, c):
        dispatch(k).wait_send()
        give_back(k).wait_send()
        return c

    with jax.named_scope("w_sent"):
        lax.fori_loop(1, n_ep, sent, 0)

    def sent_group(g, c):
        reduce_pair(g).wait_send()
        for n in range(2):
            reduce_core(g, n).wait_send()
        return c

    lax.fori_loop(0, groups, sent_group, 0)

    def spread_sent(g, c):
        if near == 0:
            spread_pair(g).wait_send()
        for n in range(2):
            spread_core(g, n).wait_send()
        return c

    lax.fori_loop(1 if single else 0, groups, spread_sent, 0)
    if near:
        for g in range(near, groups):
            spread_pair(g).wait_send()
    for k in range(1, near):
        dispatch_wide(k).wait_send()


def local(
    n_ep,
    n_tp,
    filter_value,
    filter_gate,
    filter_taps,
    filter_bias,
    norm_gain,
    norm_shift,
    out_weight,
    out_bias,
    expert_input,
    expert_gain,
    route_experts,
    route_weights,
    gate_weights,
    up_weights,
    down_weights,
):
    assert n_tp == 4 and n_ep & (n_ep - 1) == 0
    tokens, width = expert_input.shape
    capacity = 2 * tokens * route_experts.shape[1] // n_ep
    rows_all = n_ep * capacity
    group_rows = max(128, capacity)
    groups = rows_all // group_rows
    cols = width // n_tp
    length, channels = filter_value.shape
    units = gate_weights.shape[2]
    rim = -(-(filter_taps.shape[0] - 1) // 16) * 16
    vmem = pl.BlockSpec(memory_space=pltpu.VMEM)
    hbm = pl.BlockSpec(memory_space=pltpu.HBM)
    dma = pltpu.SemaphoreType.DMA
    operands = (
        filter_value,
        filter_gate,
        filter_taps,
        filter_bias[None],
        norm_gain[None],
        norm_shift[None],
        out_weight,
        out_bias[None],
        expert_input,
        expert_gain[None],
        route_experts.T,
        route_weights.T,
    )
    inputs = [
        pltpu.with_memory_space_constraint(a, pltpu.HBM)
        for a in operands + (gate_weights, up_weights, down_weights)
    ]
    return tuple(
        pl.pallas_call(
            functools.partial(kernel, n_ep, n_tp, capacity),
            out_shape=(
                jax.ShapeDtypeStruct((length, out_weight.shape[1]), bf16),
                jax.ShapeDtypeStruct((tokens, cols), bf16),
            ),
            in_specs=[hbm] * 15,
            out_specs=(vmem, vmem),
            scratch_shapes=[pltpu.VMEM(a.shape, a.dtype) for a in operands]
            + [
                pltpu.VMEM((width, units), bf16),
                pltpu.VMEM((width, units), bf16),
                pltpu.VMEM((units, width), bf16),
                pltpu.VMEM((rim, channels), bf16),
                pltpu.VMEM((rim, channels), bf16),
                pltpu.VMEM((channels // LANES, rim + length, LANES), f32),
                pltpu.VMEM((length, channels), f32),
                pltpu.VMEM((length, channels), bf16),
                pltpu.VMEM((rows_all, cols), bf16),
                pltpu.VMEM((rows_all // 2, cols), bf16),
                pltpu.VMEM((n_tp, rows_all, cols), bf16),
                pltpu.VMEM((2 * group_rows, units), bf16),
                pltpu.VMEM((n_tp, rows_all, cols), bf16),
                pltpu.VMEM((2, rows_all, cols), bf16),
                pltpu.VMEM((rows_all, cols), bf16),
                pltpu.VMEM((rows_all, cols), bf16),
                pltpu.VMEM((rows_all, cols), bf16),
                pltpu.VMEM((rows_all, cols), bf16),
                pltpu.VMEM((tokens, rows_all), bf16),
                pltpu.VMEM((tokens, rows_all), bf16),
                dma((15,)),
                dma((2,)),
                dma((n_ep,)),
                dma((n_ep,)),
                dma((n_ep,)),
                dma((n_ep,)),
                dma((groups,)),
                dma((groups,)),
                dma((groups, 2)),
                dma((groups, 2)),
                dma((groups, 2)),
                dma((groups, 2)),
                dma((groups,)),
                dma((groups,)),
                dma((n_ep,)),
                dma((n_ep,)),
            ],
            compiler_params=pltpu.CompilerParams(
                has_side_effects=True, collective_id=0, vmem_limit_bytes=44 * 1024 * 1024
            ),
            name="mixer_and_experts",
        )(*inputs)
    )


def solution(mesh):
    in_specs = (
        P(("ep", "tp"), None),
        P(("ep", "tp"), None),
        P(),
        P(),
        P(),
        P(),
        P(),
        P(),
        P("ep", None),
        P(),
        P("ep", None),
        P("ep", None),
        P("ep", None, "tp"),
        P("ep", None, "tp"),
        P("ep", "tp", None),
    )
    out_specs = (P(("ep", "tp"), None), P("ep", "tp"))
    body = functools.partial(local, mesh.shape["ep"], mesh.shape["tp"])
    return jax.shard_map(body, mesh=mesh, in_specs=in_specs, out_specs=out_specs, check_vma=False)
```

```python
import functools

import jax
import jax.numpy as jnp
from jax import lax
from jax.experimental import pallas as pl
from jax.experimental.pallas import tpu as pltpu
from jax.sharding import PartitionSpec as P

epsilon = 1e-06
clamp_limit = 7.0
swish_alpha = 1.702
LANES = 128
SCHEDULE = (
    "C0 F0 D0 S1",
    "F1 F2 A1 F3",
    "A2 S2 C1 F4",
    "D1 S3 E0 B2",
    "F5 A4 C2 A3",
    "F6 D2 B4 C3",
    "A6 C4 E2 E1",
    "D4 F7 B6 A5",
    "C5 A7 C6 E4",
    "D6 D3 B7 C7",
    "E6 D7 D5 E3",
    "E7 E5",
)
f32 = jnp.float32
bf16 = jnp.bfloat16


def dot(a, b):
    return jnp.dot(a, b, preferred_element_type=f32)


def kernel(
    n_ep,
    n_tp,
    capacity,
    value_hbm,
    gate_hbm,
    taps_hbm,
    bias_hbm,
    gain_hbm,
    shift_hbm,
    out_weight_hbm,
    out_bias_hbm,
    tokens_hbm,
    expert_gain_hbm,
    route_t_hbm,
    route_weight_t_hbm,
    gate_w_hbm,
    up_w_hbm,
    down_w_hbm,
    mixer,
    expert_out_ref,
    value,
    gate,
    taps_ref,
    bias_ref,
    gain_ref,
    shift_ref,
    out_weight,
    out_bias_ref,
    tokens_ref,
    expert_gain_ref,
    route_t_ref,
    route_weight_t_ref,
    gate_w,
    up_w,
    down_w,
    halo_out,
    halo_in,
    padded,
    filtered,
    activated,
    outgoing,
    outgoing_wide,
    arrived,
    hidden,
    partial,
    half_in,
    pair_out,
    pair_in,
    summed,
    returned,
    weight_high,
    weight_low,
    expert_sum,
    load_sem,
    halo_sem,
    disp_send,
    disp_recv,
    wide_send,
    wide_recv,
    f1_send,
    f1_recv,
    f2_send,
    f2_recv,
    r1_send,
    r1_recv,
    r2_send,
    r2_recv,
    ret_send,
    ret_recv,
):
    i = lax.axis_index("ep")
    q = lax.axis_index("tp")
    q1 = q + 1 - 2 * lax.rem(q, 2)
    q2 = lax.rem(q + 2, 4)
    q3 = lax.rem(q1 + 2, 4)
    tokens, width = tokens_ref.shape
    cols = width // n_tp
    rows_all = n_ep * capacity
    group_rows = max(128, capacity)
    per_group = group_rows // capacity
    groups = rows_all // group_rows
    length, channels = value.shape
    lane_tiles = channels // LANES
    taps = taps_ref.shape[0]
    rim = halo_out.shape[0]
    single = per_group == 1
    near = n_ep // 2 if single else 0
    here = i * n_tp + q
    last = n_ep * n_tp - 1
    following = lax.rem(here + 1, n_ep * n_tp)

    def peer(k):
        other, bit = 0, 1
        while bit < n_ep:
            other = other + bit * lax.rem(i // bit + k // bit, 2)
            bit *= 2
        return other

    barrier = pltpu.get_barrier_semaphore()

    def greet(ep, tp):
        pl.semaphore_signal(
            barrier,
            inc=1,
            device_id={"ep": ep, "tp": tp},
            device_id_type=pl.DeviceIdType.MESH,
        )

    def greet_peer(k, c):
        greet(peer(k), q)
        return c

    lax.fori_loop(1, n_ep, greet_peer, 0)
    greet(i, q1)
    greet(i, q2)

    @pl.when(here > 0)
    def _():
        greet((here - 1) // n_tp, lax.rem(here - 1, n_tp))

    copies = (
        ("route", route_t_hbm, route_t_ref),
        ("tokens", tokens_hbm, tokens_ref),
        ("expert_gain", expert_gain_hbm, expert_gain_ref),
        ("value", value_hbm, value),
        ("gate", gate_hbm, gate),
        ("taps", taps_hbm, taps_ref),
        ("bias", bias_hbm, bias_ref),
        ("gain", gain_hbm, gain_ref),
        ("shift", shift_hbm, shift_ref),
        ("out_bias", out_bias_hbm, out_bias_ref),
        ("weight_t", route_weight_t_hbm, route_weight_t_ref),
        ("gate_w", gate_w_hbm.at[0], gate_w),
        ("up_w", up_w_hbm.at[0], up_w),
        ("down_w", down_w_hbm.at[0], down_w),
        ("out_weight", out_weight_hbm, out_weight),
    )
    names = [name for name, _, _ in copies]
    loads = {
        name: pltpu.make_async_copy(s, d, load_sem.at[n])
        for n, (name, s, d) in enumerate(copies)
    }
    for name in names[:11]:
        loads[name].start()

    def remote(src, dst, send, recv, ep, tp):
        return pltpu.make_async_remote_copy(
            src_ref=src,
            dst_ref=dst,
            send_sem=send,
            recv_sem=recv,
            device_id={"ep": ep, "tp": tp},
            device_id_type=pl.DeviceIdType.MESH,
        )

    def block(k):
        return pl.ds(pl.multiple_of(k * capacity, capacity), capacity)

    def group(g):
        return pl.ds(g * group_rows, group_rows)

    def dispatch(k):
        return remote(
            outgoing.at[block(k)],
            arrived.at[q, block(k)],
            disp_send,
            disp_recv.at[k],
            peer(k),
            q,
        )

    def dispatch_wide(k):
        return remote(
            outgoing_wide.at[block(k)],
            arrived.at[q2, block(k)],
            wide_send,
            wide_recv.at[k - 1],
            peer(k),
            q,
        )

    def spread_pair(g):
        at = arrived.at[q, group(g)]
        return remote(at, at, f1_send, f1_recv.at[g - near], i, q2)

    def spread_core(g, n):
        at = arrived.at[q if n == 0 else q2, group(g)]
        return remote(at, at, f2_send, f2_recv.at[g], i, q1)

    def reduce_core(g, n):
        return remote(
            partial.at[q1 if n == 0 else q3, group(g)],
            half_in.at[n, group(g)],
            r1_send,
            r1_recv.at[g],
            i,
            q1,
        )

    def reduce_pair(g):
        return remote(
            pair_out.at[group(g)], pair_in.at[group(g)], r2_send, r2_recv.at[g], i, q2
        )

    def two_halves(send, recv, rows):
        at = half_in.at[:, pl.ds(0, rows)]
        return remote(at, at, send, recv, i, q1)

    def one_piece(send, rows):
        at = pair_in.at[pl.ds(0, rows)]
        return remote(at, at, send, r2_recv.at[0], i, q2)

    def give_back(k):
        return remote(
            summed.at[block(k)],
            returned.at[block(k)],
            ret_send,
            ret_recv.at[k],
            peer(k),
            q,
        )

    halo = remote(
        halo_out, halo_in, halo_sem.at[0], halo_sem.at[1], following // n_tp, lax.rem(following, n_tp)
    )

    def lower(a, b):
        return jnp.where(a < b, 1.0, 0.0).astype(bf16)

    side = (tokens, tokens)
    row_id = lax.broadcasted_iota(jnp.int32, side, 0)
    col_id = lax.broadcasted_iota(jnp.int32, side, 1)
    experts_t = lax.broadcasted_iota(jnp.int32, (n_ep, tokens), 0)
    loads["route"].wait()
    picks_t = [route_t_ref[n : n + 1, :] for n in range(route_t_ref.shape[0])]
    hot_t = [jnp.where(experts_t == p, 1.0, 0.0) for p in picks_t]
    rank_t = dot(sum(hot_t).astype(bf16), lower(row_id, col_id))
    slot_rows = lax.broadcasted_iota(jnp.int32, (rows_all, tokens), 0).astype(f32)
    chosen = jnp.zeros((rows_all, tokens), f32)
    targets = []
    for p, h in zip(picks_t, hot_t):
        target = (jnp.bitwise_xor(p, i) * capacity).astype(f32) + jnp.sum(
            rank_t * h, 0, keepdims=True
        )
        targets.append(target)
        chosen = jnp.where(slot_rows == target, 1.0, chosen)

    with jax.named_scope("w_tok"):
        loads["tokens"].wait()
    for name in names[11:]:
        loads[name].start()
    x = tokens_ref[...].astype(f32)
    scale = lax.rsqrt(jnp.mean(x * x, 1, keepdims=True) + epsilon)
    chosen = chosen.astype(bf16)
    loads["expert_gain"].wait()

    def columns(n):
        at = pl.ds(pl.multiple_of(n * cols, cols), cols)
        return (tokens_ref[:, at].astype(f32) * scale * expert_gain_ref[:, at]).astype(bf16)

    with jax.named_scope("select"):
        outgoing[...] = dot(chosen, columns(q)).astype(bf16)
        if near:
            outgoing_wide[...] = dot(chosen[0 : near * capacity], columns(q2)).astype(bf16)
    loads["value"].wait()
    loads["gate"].wait()
    edge = pl.ds(length - rim, rim)
    halo_out[...] = (value[edge].astype(f32) * jax.nn.sigmoid(gate[edge].astype(f32))).astype(bf16)

    with jax.named_scope("w_barrier"):
        pl.semaphore_wait(barrier, n_ep + 2 - jnp.where(here == last, 1, 0))

    @pl.when(here < last)
    def _():
        halo.start()

    @pl.when(here == 0)
    def _():
        halo_in[...] = jnp.zeros_like(halo_in)

    if single and n_ep == 8:
        staged = ((1, -1, 4, 2), (5, -2), (6, 3), (7, -3))
    else:
        staged = (range(1, n_ep),)

    def send(n):
        for k in staged[n] if n < len(staged) else ():
            (dispatch(k) if k > 0 else dispatch_wide(-k)).start()

    with jax.named_scope("wide"):
        send(0)
    with jax.named_scope("own"):
        if single:
            for n in range(n_tp):
                arrived[n, 0:capacity] = dot(chosen[0:capacity], columns(n)).astype(bf16)
        else:
            arrived[q, 0:capacity] = outgoing[0:capacity]

    def gate_tile(l, c):
        at = pl.ds(pl.multiple_of(l * LANES, LANES), LANES)
        padded[l, rim:] = (
            (value[:, at].astype(f32) * jax.nn.sigmoid(gate[:, at].astype(f32)))
            .astype(bf16)
            .astype(f32)
        )
        return c

    def conv_tile(l, c):
        at = pl.ds(pl.multiple_of(l * LANES, LANES), LANES)
        padded[l, 0:rim] = halo_in[:, at].astype(f32)
        total = jnp.zeros((length, LANES), f32) + bias_ref[:, at]
        for j in range(taps):
            total = total + taps_ref[j : j + 1, at] * padded[l, pl.ds(rim - taps + 1 + j, length)]
        filtered[:, at] = total
        return c

    def norm_rows(r, c):
        at = pl.ds(pl.multiple_of(r * 32, 32), 32)
        f = filtered[at]
        centred = f - jnp.mean(f, 1, keepdims=True)
        variance = jnp.mean(centred * centred, 1, keepdims=True)
        v = centred * lax.rsqrt(variance + epsilon) * gain_ref[...] + shift_ref[...]
        activated[at] = (v * jax.nn.sigmoid(v)).astype(bf16)
        return c

    def project(n, c):
        at = pl.ds(pl.multiple_of(n * 256, 256), 256)
        mixer[:, at] = (dot(activated[...], out_weight[:, at]) + out_bias_ref[:, at]).astype(bf16)
        return c

    def experts_of(gs):
        ats = [group(g) for g in gs]
        held_rows = pl.ds(0, len(gs) * group_rows)

        def unit(n, c):
            u_at = pl.ds(pl.multiple_of(n * 256, 256), 256)
            rows = jnp.concatenate(
                [jnp.concatenate([arrived[s, at] for s in range(n_tp)], 1) for at in ats], 0
            )
            g_pre = dot(rows, gate_w[:, u_at])
            u_pre = dot(rows, up_w[:, u_at])
            held = jnp.minimum(g_pre, clamp_limit)
            up = jnp.clip(u_pre, -clamp_limit, clamp_limit)
            hidden[held_rows, u_at] = (held * jax.nn.sigmoid(swish_alpha * held) * (up + 1.0)).astype(bf16)
            return c

        lax.fori_loop(0, gate_w.shape[1] // 256, unit, 0)

        def down(s, c):
            at_cols = pl.ds(pl.multiple_of(s * cols, cols), cols)
            part = dot(hidden[held_rows, :], down_w[:, at_cols]).astype(bf16)
            for n, at in enumerate(ats):
                partial[s, at] = part[n * group_rows : (n + 1) * group_rows]
            return c

        lax.fori_loop(0, n_tp, down, 0)

    def arrive(k, c):
        dispatch(k).wait_recv()
        return c

    def give(k, c):
        give_back(k).start()
        return c

    if single and n_ep == 8:
        order = [0, 1, 4, 2, 5, 3, 6, 7]
    else:
        order = list(range(groups))
    wide = [g < near for g in order]

    def take(s):
        g = order[s]
        if single and s == 0:
            return
        with jax.named_scope(f"A{s}"):
            lax.fori_loop(jnp.maximum(g * per_group, 1), (g + 1) * per_group, arrive, 0)
            if wide[s]:
                dispatch_wide(g).wait_recv()
            else:
                spread_pair(g).start()
            spread_core(g, 0).start()
            if wide[s]:
                spread_core(g, 1).start()

    def relay(s):
        g = order[s]
        if wide[s]:
            return
        with jax.named_scope(f"B{s}"):
            spread_pair(g).wait_recv()
            spread_core(g, 1).start()

    def compute(*steps):
        for s in steps:
            if not (single and s == 0):
                with jax.named_scope(f"Cw{s}"):
                    two_halves(f2_send, f2_recv.at[order[s]], group_rows).wait_recv()
        with jax.named_scope(f"C{steps}"):
            experts_of([order[s] for s in steps])
        for s in steps:
            reduce_core(order[s], 0).start()
            reduce_core(order[s], 1).start()

    def halve(s):
        g = order[s]
        at = group(g)
        with jax.named_scope(f"D{s}"):
            two_halves(r1_send, r1_recv.at[g], group_rows).wait_recv()
            pair_out[at] = (partial[q2, at].astype(f32) + half_in[1, at].astype(f32)).astype(bf16)
            reduce_pair(g).start()

    def finish(s):
        g = order[s]
        at = group(g)
        with jax.named_scope(f"E{s}"):
            reduce_pair(g).wait_recv()
            summed[at] = (
                partial[q, at].astype(f32) + half_in[0, at].astype(f32) + pair_in[at].astype(f32)
            ).astype(bf16)
            lax.fori_loop(jnp.maximum(g * per_group, 1), (g + 1) * per_group, give, 0)

    def mixer_gate():
        lax.fori_loop(0, lane_tiles, gate_tile, 0)

    def mixer_halo():
        for name in ("taps", "bias", "gain", "shift"):
            loads[name].wait()

        @pl.when(here > 0)
        def _():
            halo.wait_recv()

    def mixer_conv(n):
        lax.fori_loop(n * lane_tiles // 2, (n + 1) * lane_tiles // 2, conv_tile, 0)

    def mixer_norm():
        lax.fori_loop(0, length // 32, norm_rows, 0)

    def mixer_project(n):
        if n == 0:
            loads["out_weight"].wait()
            loads["out_bias"].wait()
        tiles = out_weight.shape[1] // 256
        lax.fori_loop(n * tiles // 2, (n + 1) * tiles // 2, project, 0)

    def weigh():
        loads["weight_t"].wait()
        weights = jnp.zeros((rows_all, tokens), f32)
        for n, target in enumerate(targets):
            weights = jnp.where(slot_rows == target, route_weight_t_ref[n : n + 1, :], weights)
        weights = weights.T
        high = weights.astype(bf16)
        weight_high[...] = high
        weight_low[...] = (weights - high.astype(f32)).astype(bf16)

    fillers = [
        mixer_gate,
        mixer_halo,
        functools.partial(mixer_conv, 0),
        functools.partial(mixer_conv, 1),
        mixer_norm,
        functools.partial(mixer_project, 0),
        functools.partial(mixer_project, 1),
        weigh,
    ]

    def fill(n):
        with jax.named_scope(f"F{n}"):
            fillers[n]()

    for name in ("gate_w", "up_w", "down_w"):
        loads[name].wait()
    stages = {"A": take, "B": relay, "S": send, "C": compute, "D": halve, "E": finish, "F": fill}
    for word in " ".join(SCHEDULE).split():
        stages[word[0]](*[int(n) for n in word[1:].split("+")])
    returned[0:capacity] = summed[0:capacity]

    def came_back(k, c):
        give_back(k).wait_recv()
        return c

    def weighted(low, high):
        at = pl.ds(low * capacity, (high - low) * capacity)
        return dot(weight_high[:, at], returned[at]) + dot(weight_low[:, at], returned[at])

    with jax.named_scope("w_ret"):
        if single:
            final = order[-1]
            lax.fori_loop(1, final, came_back, 0)
            expert_sum[...] = weighted(0, final)
            came_back(final, 0)
        else:
            lax.fori_loop(1, n_ep, came_back, 0)
    with jax.named_scope("final"):
        if single:
            expert_out_ref[...] = (expert_sum[...] + weighted(final, n_ep)).astype(bf16)
        else:
            expert_out_ref[...] = weighted(0, n_ep).astype(bf16)

    @pl.when(here < last)
    def _():
        halo.wait_send()

    lead = group_rows if single else 0
    with jax.named_scope("w_sent"):
        one_piece(disp_send, rows_all - capacity).wait_send()
        one_piece(ret_send, rows_all - capacity).wait_send()
        one_piece(r2_send, rows_all).wait_send()
        one_piece(f1_send, rows_all - near * group_rows).wait_send()
        two_halves(r1_send, r1_recv.at[0], rows_all).wait_send()
        two_halves(f2_send, f2_recv.at[0], rows_all - lead).wait_send()
        if near:
            one_piece(wide_send, (near - 1) * capacity).wait_send()


def publish(mixer, expert, mixer_hbm, expert_hbm, sems):
    copies = [
        pltpu.make_async_copy(mixer, mixer_hbm, sems.at[0]),
        pltpu.make_async_copy(expert, expert_hbm, sems.at[1]),
    ]
    for copy in copies:
        copy.start()
    for copy in copies:
        copy.wait()


def local(
    n_ep,
    n_tp,
    filter_value,
    filter_gate,
    filter_taps,
    filter_bias,
    norm_gain,
    norm_shift,
    out_weight,
    out_bias,
    expert_input,
    expert_gain,
    route_experts,
    route_weights,
    gate_weights,
    up_weights,
    down_weights,
):
    assert n_tp == 4 and n_ep & (n_ep - 1) == 0
    tokens, width = expert_input.shape
    capacity = 2 * tokens * route_experts.shape[1] // n_ep
    rows_all = n_ep * capacity
    group_rows = max(128, capacity)
    groups = rows_all // group_rows
    cols = width // n_tp
    length, channels = filter_value.shape
    units = gate_weights.shape[2]
    rim = -(-(filter_taps.shape[0] - 1) // 16) * 16
    vmem = pl.BlockSpec(memory_space=pltpu.VMEM)
    hbm = pl.BlockSpec(memory_space=pltpu.HBM)
    dma = pltpu.SemaphoreType.DMA
    operands = (
        filter_value,
        filter_gate,
        filter_taps,
        filter_bias[None],
        norm_gain[None],
        norm_shift[None],
        out_weight,
        out_bias[None],
        expert_input,
        expert_gain[None],
        route_experts.T,
        route_weights.T,
    )
    inputs = [
        pltpu.with_memory_space_constraint(a, pltpu.HBM)
        for a in operands + (gate_weights, up_weights, down_weights)
    ]
    results = (
        jax.ShapeDtypeStruct((length, out_weight.shape[1]), bf16),
        jax.ShapeDtypeStruct((tokens, cols), bf16),
    )
    mixed, expert_out = (
        pl.pallas_call(
            functools.partial(kernel, n_ep, n_tp, capacity),
            out_shape=results,
            in_specs=[hbm] * 15,
            out_specs=(vmem, vmem),
            scratch_shapes=[pltpu.VMEM(a.shape, a.dtype) for a in operands]
            + [
                pltpu.VMEM((width, units), bf16),
                pltpu.VMEM((width, units), bf16),
                pltpu.VMEM((units, width), bf16),
                pltpu.VMEM((rim, channels), bf16),
                pltpu.VMEM((rim, channels), bf16),
                pltpu.VMEM((channels // LANES, rim + length, LANES), f32),
                pltpu.VMEM((length, channels), f32),
                pltpu.VMEM((length, channels), bf16),
                pltpu.VMEM((rows_all, cols), bf16),
                pltpu.VMEM((rows_all // 2, cols), bf16),
                pltpu.VMEM((n_tp, rows_all, cols), bf16),
                pltpu.VMEM((2 * group_rows, units), bf16),
                pltpu.VMEM((n_tp, rows_all, cols), bf16),
                pltpu.VMEM((2, rows_all, cols), bf16),
                pltpu.VMEM((rows_all, cols), bf16),
                pltpu.VMEM((rows_all, cols), bf16),
                pltpu.VMEM((rows_all, cols), bf16),
                pltpu.VMEM((rows_all, cols), bf16),
                pltpu.VMEM((tokens, rows_all), bf16),
                pltpu.VMEM((tokens, rows_all), bf16),
                pltpu.VMEM((tokens, cols), f32),
                dma((15,)),
                dma((2,)),
                dma,
                dma((n_ep,)),
                dma,
                dma((n_ep // 2,)),
                dma,
                dma((groups,)),
                dma,
                dma((groups,)),
                dma,
                dma((groups,)),
                dma,
                dma((groups,)),
                dma,
                dma((n_ep,)),
            ],
            compiler_params=pltpu.CompilerParams(
                has_side_effects=True, collective_id=0, vmem_limit_bytes=44 * 1024 * 1024
            ),
            name="mixer_and_experts",
        )(*inputs)
    )
    return tuple(
        pl.pallas_call(
            publish,
            out_shape=results,
            in_specs=[vmem] * 2,
            out_specs=(hbm, hbm),
            scratch_shapes=[dma((2,))],
            compiler_params=pltpu.CompilerParams(vmem_limit_bytes=1024 * 1024),
            name="publish",
        )(mixed, expert_out)
    )


def solution(mesh):
    in_specs = (
        P(("ep", "tp"), None),
        P(("ep", "tp"), None),
        P(),
        P(),
        P(),
        P(),
        P(),
        P(),
        P("ep", None),
        P(),
        P("ep", None),
        P("ep", None),
        P("ep", None, "tp"),
        P("ep", None, "tp"),
        P("ep", "tp", None),
    )
    out_specs = (P(("ep", "tp"), None), P("ep", "tp"))
    body = functools.partial(local, mesh.shape["ep"], mesh.shape["tp"])
    return jax.shard_map(body, mesh=mesh, in_specs=in_specs, out_specs=out_specs, check_vma=False)
```

```python
import functools

import jax
import jax.numpy as jnp
from jax import lax
from jax.experimental import pallas as pl
from jax.experimental.pallas import tpu as pltpu
from jax.sharding import PartitionSpec as P

epsilon = 1e-06
clamp_limit = 7.0
swish_alpha = 1.702
LANES = 128
SCHEDULE = (
    "H G1 W1 G4",
    "G2 O R C0",
    "F0 D0 G5 W2",
    "F1 F2 A1 F3",
    "A2 G6 G3 G7",
    "C1 F4 D1 W3",
    "E0 B2 F5 A4",
    "C2 A3 F6 D2",
    "B4 A6 C3+4 E2",
    "E1 A5 D4 F7",
    "B6 A7 C5+6 E4",
    "D6 D3 B7 C7",
    "E6 D5 D7 E3",
    "E5 E7",
)
f32 = jnp.float32
bf16 = jnp.bfloat16


def dot(a, b):
    return jnp.dot(a, b, preferred_element_type=f32)


def plain_schedule(n_ep, groups):
    words = ["H"] + [f"G{k}" for k in range(1, n_ep)] + "O R F0 F1 F2 F3 F4 F5 F6 F7".split()
    for t in range(groups + 4):
        for stage, lag in (("D", 3), ("E", 4), ("B", 1), ("C", 2), ("A", 0)):
            if 0 <= t - lag < groups:
                words.append(f"{stage}{t - lag}")
    return words


def kernel(
    n_ep,
    n_tp,
    capacity,
    value_hbm,
    gate_hbm,
    taps_hbm,
    bias_hbm,
    gain_hbm,
    shift_hbm,
    out_weight_hbm,
    out_bias_hbm,
    tokens_hbm,
    expert_gain_hbm,
    route_t_hbm,
    route_weight_t_hbm,
    gate_w_hbm,
    up_w_hbm,
    down_w_hbm,
    mixer,
    expert_out_ref,
    value,
    gate,
    taps_ref,
    bias_ref,
    gain_ref,
    shift_ref,
    out_weight,
    out_bias_ref,
    tokens_ref,
    expert_gain_ref,
    route_t_ref,
    route_weight_t_ref,
    gate_w,
    up_w,
    down_w,
    halo_out,
    halo_in,
    padded,
    filtered,
    activated,
    outgoing,
    outgoing_wide,
    arrived,
    hidden,
    partial,
    half_in,
    pair_out,
    pair_in,
    summed,
    returned,
    weight_high,
    weight_low,
    expert_sum,
    load_sem,
    halo_sem,
    disp_send,
    disp_recv,
    wide_send,
    wide_recv,
    f1_send,
    f1_recv,
    f2_send,
    f2_recv,
    r1_send,
    r1_recv,
    r2_send,
    r2_recv,
    ret_send,
    ret_recv,
):
    i = lax.axis_index("ep")
    q = lax.axis_index("tp")
    q1 = q + 1 - 2 * lax.rem(q, 2)
    q2 = lax.rem(q + 2, 4)
    q3 = lax.rem(q1 + 2, 4)
    tokens, width = tokens_ref.shape
    cols = width // n_tp
    rows_all = n_ep * capacity
    group_rows = max(128, capacity)
    per_group = group_rows // capacity
    groups = rows_all // group_rows
    length, channels = value.shape
    lane_tiles = channels // LANES
    taps = taps_ref.shape[0]
    rim = halo_out.shape[0]
    single = per_group == 1
    near = n_ep // 2 if single else 0
    here = i * n_tp + q
    last = n_ep * n_tp - 1
    following = lax.rem(here + 1, n_ep * n_tp)

    def peer(k):
        other, bit = 0, 1
        while bit < n_ep:
            other = other + bit * lax.rem(i // bit + k // bit, 2)
            bit *= 2
        return other

    barrier = pltpu.get_barrier_semaphore()

    def greet(ep, tp):
        pl.semaphore_signal(
            barrier,
            inc=1,
            device_id={"ep": ep, "tp": tp},
            device_id_type=pl.DeviceIdType.MESH,
        )

    def greet_peer(k, c):
        greet(peer(k), q)
        return c

    lax.fori_loop(1, n_ep, greet_peer, 0)
    greet(i, q1)
    greet(i, q2)

    @pl.when(here > 0)
    def _():
        greet((here - 1) // n_tp, lax.rem(here - 1, n_tp))

    copies = (
        ("route", route_t_hbm, route_t_ref),
        ("tokens", tokens_hbm, tokens_ref),
        ("expert_gain", expert_gain_hbm, expert_gain_ref),
        ("value", value_hbm, value),
        ("gate", gate_hbm, gate),
        ("taps", taps_hbm, taps_ref),
        ("bias", bias_hbm, bias_ref),
        ("gain", gain_hbm, gain_ref),
        ("shift", shift_hbm, shift_ref),
        ("out_bias", out_bias_hbm, out_bias_ref),
        ("weight_t", route_weight_t_hbm, route_weight_t_ref),
        ("gate_w", gate_w_hbm.at[0], gate_w),
        ("up_w", up_w_hbm.at[0], up_w),
        ("down_w", down_w_hbm.at[0], down_w),
        ("out_weight", out_weight_hbm, out_weight),
    )
    names = [name for name, _, _ in copies]
    loads = {
        name: pltpu.make_async_copy(s, d, load_sem.at[n])
        for n, (name, s, d) in enumerate(copies)
    }
    for name in names[:11]:
        loads[name].start()

    def remote(src, dst, send, recv, ep, tp):
        return pltpu.make_async_remote_copy(
            src_ref=src,
            dst_ref=dst,
            send_sem=send,
            recv_sem=recv,
            device_id={"ep": ep, "tp": tp},
            device_id_type=pl.DeviceIdType.MESH,
        )

    def block(k):
        return pl.ds(pl.multiple_of(k * capacity, capacity), capacity)

    def group(g):
        return pl.ds(g * group_rows, group_rows)

    def dispatch(k):
        return remote(
            outgoing.at[block(k)],
            arrived.at[q, block(k)],
            disp_send,
            disp_recv.at[k],
            peer(k),
            q,
        )

    def dispatch_wide(k):
        return remote(
            outgoing_wide.at[block(k)],
            arrived.at[q2, block(k)],
            wide_send,
            wide_recv.at[k - 1],
            peer(k),
            q,
        )

    def spread_pair(g):
        at = arrived.at[q, group(g)]
        return remote(at, at, f1_send, f1_recv.at[g - near], i, q2)

    def spread_core(g, n):
        at = arrived.at[q if n == 0 else q2, group(g)]
        return remote(at, at, f2_send, f2_recv.at[g], i, q1)

    def reduce_core(g, n):
        return remote(
            partial.at[q1 if n == 0 else q3, group(g)],
            half_in.at[n, group(g)],
            r1_send,
            r1_recv.at[g],
            i,
            q1,
        )

    def reduce_pair(g):
        return remote(
            pair_out.at[group(g)], pair_in.at[group(g)], r2_send, r2_recv.at[g], i, q2
        )

    def two_halves(send, recv, rows):
        at = half_in.at[:, pl.ds(0, rows)]
        return remote(at, at, send, recv, i, q1)

    def one_piece(send, rows):
        at = pair_in.at[pl.ds(0, rows)]
        return remote(at, at, send, r2_recv.at[0], i, q2)

    def give_back(k):
        return remote(
            summed.at[block(k)],
            returned.at[block(k)],
            ret_send,
            ret_recv.at[k],
            peer(k),
            q,
        )

    halo = remote(
        halo_out, halo_in, halo_sem.at[0], halo_sem.at[1], following // n_tp, lax.rem(following, n_tp)
    )

    def lower(a, b):
        return jnp.where(a < b, 1.0, 0.0).astype(bf16)

    side = (tokens, tokens)
    row_id = lax.broadcasted_iota(jnp.int32, side, 0)
    col_id = lax.broadcasted_iota(jnp.int32, side, 1)
    experts_t = lax.broadcasted_iota(jnp.int32, (n_ep, tokens), 0)
    loads["route"].wait()
    picks_t = [route_t_ref[n : n + 1, :] for n in range(route_t_ref.shape[0])]
    hot_t = [jnp.where(experts_t == p, 1.0, 0.0) for p in picks_t]
    rank_t = dot(sum(hot_t).astype(bf16), lower(row_id, col_id))
    slot_rows = lax.broadcasted_iota(jnp.int32, (rows_all, tokens), 0).astype(f32)
    chosen = jnp.zeros((rows_all, tokens), f32)
    targets = []
    for p, h in zip(picks_t, hot_t):
        target = (jnp.bitwise_xor(p, i) * capacity).astype(f32) + jnp.sum(
            rank_t * h, 0, keepdims=True
        )
        targets.append(target)
        chosen = jnp.where(slot_rows == target, 1.0, chosen)

    with jax.named_scope("w_tok"):
        loads["tokens"].wait()
    for name in names[11:]:
        loads[name].start()
    x = tokens_ref[...].astype(f32)
    scale = lax.rsqrt(jnp.mean(x * x, 1, keepdims=True) + epsilon)
    chosen = chosen.astype(bf16)
    loads["expert_gain"].wait()

    def columns(n):
        at = pl.ds(pl.multiple_of(n * cols, cols), cols)
        return (tokens_ref[:, at].astype(f32) * scale * expert_gain_ref[:, at]).astype(bf16)

    with jax.named_scope("select"):
        outgoing[...] = dot(chosen, columns(q)).astype(bf16)
        if near:
            outgoing_wide[...] = dot(chosen[0 : near * capacity], columns(q2)).astype(bf16)
    loads["value"].wait()
    loads["gate"].wait()
    edge = pl.ds(length - rim, rim)
    halo_out[...] = (value[edge].astype(f32) * jax.nn.sigmoid(gate[edge].astype(f32))).astype(bf16)

    with jax.named_scope("w_barrier"):
        pl.semaphore_wait(barrier, n_ep + 2 - jnp.where(here == last, 1, 0))

    @pl.when(here == 0)
    def _():
        halo_in[...] = jnp.zeros_like(halo_in)

    def start_halo():
        @pl.when(here < last)
        def _():
            halo.start()

    def send(k):
        dispatch(k).start()

    def send_wide(k):
        dispatch_wide(k).start()

    def own():
        with jax.named_scope("own"):
            if single:
                for n in range(n_tp):
                    arrived[n, 0:capacity] = dot(chosen[0:capacity], columns(n)).astype(bf16)
            else:
                arrived[q, 0:capacity] = outgoing[0:capacity]

    def gate_tile(l, c):
        at = pl.ds(pl.multiple_of(l * LANES, LANES), LANES)
        padded[l, rim:] = (
            (value[:, at].astype(f32) * jax.nn.sigmoid(gate[:, at].astype(f32)))
            .astype(bf16)
            .astype(f32)
        )
        return c

    def conv_tile(l, c):
        at = pl.ds(pl.multiple_of(l * LANES, LANES), LANES)
        padded[l, 0:rim] = halo_in[:, at].astype(f32)
        total = jnp.zeros((length, LANES), f32) + bias_ref[:, at]
        for j in range(taps):
            total = total + taps_ref[j : j + 1, at] * padded[l, pl.ds(rim - taps + 1 + j, length)]
        filtered[:, at] = total
        return c

    def norm_rows(r, c):
        at = pl.ds(pl.multiple_of(r * 32, 32), 32)
        f = filtered[at]
        centred = f - jnp.mean(f, 1, keepdims=True)
        variance = jnp.mean(centred * centred, 1, keepdims=True)
        v = centred * lax.rsqrt(variance + epsilon) * gain_ref[...] + shift_ref[...]
        activated[at] = (v * jax.nn.sigmoid(v)).astype(bf16)
        return c

    def project(n, c):
        at = pl.ds(pl.multiple_of(n * 256, 256), 256)
        mixer[:, at] = (dot(activated[...], out_weight[:, at]) + out_bias_ref[:, at]).astype(bf16)
        return c

    def experts_of(gs):
        ats = [group(g) for g in gs]
        held_rows = pl.ds(0, len(gs) * group_rows)

        def unit(n, c):
            u_at = pl.ds(pl.multiple_of(n * 256, 256), 256)
            rows = jnp.concatenate(
                [jnp.concatenate([arrived[s, at] for s in range(n_tp)], 1) for at in ats], 0
            )
            g_pre = dot(rows, gate_w[:, u_at])
            u_pre = dot(rows, up_w[:, u_at])
            held = jnp.minimum(g_pre, clamp_limit)
            up = jnp.clip(u_pre, -clamp_limit, clamp_limit)
            hidden[held_rows, u_at] = (held * jax.nn.sigmoid(swish_alpha * held) * (up + 1.0)).astype(bf16)
            return c

        lax.fori_loop(0, gate_w.shape[1] // 256, unit, 0)

        def down(s, c):
            at_cols = pl.ds(pl.multiple_of(s * cols, cols), cols)
            part = dot(hidden[held_rows, :], down_w[:, at_cols]).astype(bf16)
            for n, at in enumerate(ats):
                partial[s, at] = part[n * group_rows : (n + 1) * group_rows]
            return c

        lax.fori_loop(0, n_tp, down, 0)

    def arrive(k, c):
        dispatch(k).wait_recv()
        return c

    def give(k, c):
        give_back(k).start()
        return c

    if single and n_ep == 8:
        order = [0, 1, 4, 2, 5, 3, 6, 7]
    else:
        order = list(range(groups))
    wide = [g < near for g in order]

    def take(s):
        g = order[s]
        if single and s == 0:
            return
        with jax.named_scope(f"A{s}"):
            lax.fori_loop(jnp.maximum(g * per_group, 1), (g + 1) * per_group, arrive, 0)
            if wide[s]:
                dispatch_wide(g).wait_recv()
            else:
                spread_pair(g).start()
            spread_core(g, 0).start()
            if wide[s]:
                spread_core(g, 1).start()

    def relay(s):
        g = order[s]
        if wide[s]:
            return
        with jax.named_scope(f"B{s}"):
            spread_pair(g).wait_recv()
            spread_core(g, 1).start()

    def compute(*steps):
        for s in steps:
            if not (single and s == 0):
                with jax.named_scope(f"Cw{s}"):
                    two_halves(f2_send, f2_recv.at[order[s]], group_rows).wait_recv()
        with jax.named_scope(f"C{steps}"):
            experts_of([order[s] for s in steps])
        for s in steps:
            reduce_core(order[s], 0).start()
            reduce_core(order[s], 1).start()

    def halve(s):
        g = order[s]
        at = group(g)
        with jax.named_scope(f"D{s}"):
            two_halves(r1_send, r1_recv.at[g], group_rows).wait_recv()
            pair_out[at] = (partial[q2, at].astype(f32) + half_in[1, at].astype(f32)).astype(bf16)
            reduce_pair(g).start()

    def finish(s):
        g = order[s]
        at = group(g)
        with jax.named_scope(f"E{s}"):
            reduce_pair(g).wait_recv()
            summed[at] = (
                partial[q, at].astype(f32) + half_in[0, at].astype(f32) + pair_in[at].astype(f32)
            ).astype(bf16)
            lax.fori_loop(jnp.maximum(g * per_group, 1), (g + 1) * per_group, give, 0)

    def mixer_gate():
        lax.fori_loop(0, lane_tiles, gate_tile, 0)

    def mixer_halo():
        for name in ("taps", "bias", "gain", "shift"):
            loads[name].wait()

        @pl.when(here > 0)
        def _():
            halo.wait_recv()

    def mixer_conv(n):
        lax.fori_loop(n * lane_tiles // 2, (n + 1) * lane_tiles // 2, conv_tile, 0)

    def mixer_norm():
        lax.fori_loop(0, length // 32, norm_rows, 0)

    def mixer_project(n):
        if n == 0:
            loads["out_weight"].wait()
            loads["out_bias"].wait()
        tiles = out_weight.shape[1] // 256
        lax.fori_loop(n * tiles // 2, (n + 1) * tiles // 2, project, 0)

    def weigh():
        loads["weight_t"].wait()
        weights = jnp.zeros((rows_all, tokens), f32)
        for n, target in enumerate(targets):
            weights = jnp.where(slot_rows == target, route_weight_t_ref[n : n + 1, :], weights)
        weights = weights.T
        high = weights.astype(bf16)
        weight_high[...] = high
        weight_low[...] = (weights - high.astype(f32)).astype(bf16)

    fillers = [
        mixer_gate,
        mixer_halo,
        functools.partial(mixer_conv, 0),
        functools.partial(mixer_conv, 1),
        mixer_norm,
        functools.partial(mixer_project, 0),
        functools.partial(mixer_project, 1),
        weigh,
    ]

    def fill(n):
        with jax.named_scope(f"F{n}"):
            fillers[n]()

    def ready():
        for name in ("gate_w", "up_w", "down_w"):
            loads[name].wait()

    once = {"H": start_halo, "O": own, "R": ready}
    stages = {"A": take, "B": relay, "G": send, "W": send_wide, "C": compute, "D": halve, "E": finish, "F": fill}
    for word in " ".join(SCHEDULE).split() if single and n_ep == 8 else plain_schedule(n_ep, groups):
        if word in once:
            once[word]()
        else:
            stages[word[0]](*[int(n) for n in word[1:].split("+")])
    returned[0:capacity] = summed[0:capacity]

    def came_back(k, c):
        give_back(k).wait_recv()
        return c

    def weighted(low, high):
        at = pl.ds(low * capacity, (high - low) * capacity)
        return dot(weight_high[:, at], returned[at]) + dot(weight_low[:, at], returned[at])

    with jax.named_scope("w_ret"):
        if single:
            final = order[-1]
            lax.fori_loop(1, final, came_back, 0)
            expert_sum[...] = weighted(0, final)
            came_back(final, 0)
        else:
            lax.fori_loop(1, n_ep, came_back, 0)
    with jax.named_scope("final"):
        if single:
            expert_out_ref[...] = (expert_sum[...] + weighted(final, n_ep)).astype(bf16)
        else:
            expert_out_ref[...] = weighted(0, n_ep).astype(bf16)

    @pl.when(here < last)
    def _():
        halo.wait_send()

    lead = group_rows if single else 0
    with jax.named_scope("w_sent"):
        one_piece(disp_send, rows_all - capacity).wait_send()
        one_piece(ret_send, rows_all - capacity).wait_send()
        one_piece(r2_send, rows_all).wait_send()
        one_piece(f1_send, rows_all - near * group_rows).wait_send()
        two_halves(r1_send, r1_recv.at[0], rows_all).wait_send()
        two_halves(f2_send, f2_recv.at[0], rows_all - lead).wait_send()
        if near:
            one_piece(wide_send, (near - 1) * capacity).wait_send()


def publish(mixer, expert, mixer_hbm, expert_hbm, sems):
    copies = [
        pltpu.make_async_copy(mixer, mixer_hbm, sems.at[0]),
        pltpu.make_async_copy(expert, expert_hbm, sems.at[1]),
    ]
    for copy in copies:
        copy.start()
    for copy in copies:
        copy.wait()


def local(
    n_ep,
    n_tp,
    filter_value,
    filter_gate,
    filter_taps,
    filter_bias,
    norm_gain,
    norm_shift,
    out_weight,
    out_bias,
    expert_input,
    expert_gain,
    route_experts,
    route_weights,
    gate_weights,
    up_weights,
    down_weights,
):
    assert n_tp == 4 and n_ep & (n_ep - 1) == 0
    tokens, width = expert_input.shape
    capacity = 2 * tokens * route_experts.shape[1] // n_ep
    rows_all = n_ep * capacity
    group_rows = max(128, capacity)
    groups = rows_all // group_rows
    cols = width // n_tp
    length, channels = filter_value.shape
    units = gate_weights.shape[2]
    rim = -(-(filter_taps.shape[0] - 1) // 16) * 16
    vmem = pl.BlockSpec(memory_space=pltpu.VMEM)
    hbm = pl.BlockSpec(memory_space=pltpu.HBM)
    dma = pltpu.SemaphoreType.DMA
    operands = (
        filter_value,
        filter_gate,
        filter_taps,
        filter_bias[None],
        norm_gain[None],
        norm_shift[None],
        out_weight,
        out_bias[None],
        expert_input,
        expert_gain[None],
        route_experts.T,
        route_weights.T,
    )
    inputs = [
        pltpu.with_memory_space_constraint(a, pltpu.HBM)
        for a in operands + (gate_weights, up_weights, down_weights)
    ]
    results = (
        jax.ShapeDtypeStruct((length, out_weight.shape[1]), bf16),
        jax.ShapeDtypeStruct((tokens, cols), bf16),
    )
    mixed, expert_out = (
        pl.pallas_call(
            functools.partial(kernel, n_ep, n_tp, capacity),
            out_shape=results,
            in_specs=[hbm] * 15,
            out_specs=(vmem, vmem),
            scratch_shapes=[pltpu.VMEM(a.shape, a.dtype) for a in operands]
            + [
                pltpu.VMEM((width, units), bf16),
                pltpu.VMEM((width, units), bf16),
                pltpu.VMEM((units, width), bf16),
                pltpu.VMEM((rim, channels), bf16),
                pltpu.VMEM((rim, channels), bf16),
                pltpu.VMEM((channels // LANES, rim + length, LANES), f32),
                pltpu.VMEM((length, channels), f32),
                pltpu.VMEM((length, channels), bf16),
                pltpu.VMEM((rows_all, cols), bf16),
                pltpu.VMEM((rows_all // 2, cols), bf16),
                pltpu.VMEM((n_tp, rows_all, cols), bf16),
                pltpu.VMEM((2 * group_rows, units), bf16),
                pltpu.VMEM((n_tp, rows_all, cols), bf16),
                pltpu.VMEM((2, rows_all, cols), bf16),
                pltpu.VMEM((rows_all, cols), bf16),
                pltpu.VMEM((rows_all, cols), bf16),
                pltpu.VMEM((rows_all, cols), bf16),
                pltpu.VMEM((rows_all, cols), bf16),
                pltpu.VMEM((tokens, rows_all), bf16),
                pltpu.VMEM((tokens, rows_all), bf16),
                pltpu.VMEM((tokens, cols), f32),
                dma((15,)),
                dma((2,)),
                dma,
                dma((n_ep,)),
                dma,
                dma((n_ep // 2,)),
                dma,
                dma((groups,)),
                dma,
                dma((groups,)),
                dma,
                dma((groups,)),
                dma,
                dma((groups,)),
                dma,
                dma((n_ep,)),
            ],
            compiler_params=pltpu.CompilerParams(
                has_side_effects=True, collective_id=0, vmem_limit_bytes=44 * 1024 * 1024
            ),
            name="mixer_and_experts",
        )(*inputs)
    )
    return tuple(
        pl.pallas_call(
            publish,
            out_shape=results,
            in_specs=[vmem] * 2,
            out_specs=(hbm, hbm),
            scratch_shapes=[dma((2,))],
            compiler_params=pltpu.CompilerParams(vmem_limit_bytes=1024 * 1024),
            name="publish",
        )(mixed, expert_out)
    )


def solution(mesh):
    in_specs = (
        P(("ep", "tp"), None),
        P(("ep", "tp"), None),
        P(),
        P(),
        P(),
        P(),
        P(),
        P(),
        P("ep", None),
        P(),
        P("ep", None),
        P("ep", None),
        P("ep", None, "tp"),
        P("ep", None, "tp"),
        P("ep", "tp", None),
    )
    out_specs = (P(("ep", "tp"), None), P("ep", "tp"))
    body = functools.partial(local, mesh.shape["ep"], mesh.shape["tp"])
    return jax.shard_map(body, mesh=mesh, in_specs=in_specs, out_specs=out_specs, check_vma=False)
```

```python
import functools

import jax
import jax.numpy as jnp
from jax import lax
from jax.experimental import pallas as pl
from jax.experimental.pallas import tpu as pltpu
from jax.sharding import PartitionSpec as P

epsilon = 1e-06
clamp_limit = 7.0
swish_alpha = 1.702
LANES = 128
SCHEDULE = (
    "H G1 W1 G4",
    "G2 O R C0",
    "F0 D0 G5 W2",
    "F1 F2 A1 F3",
    "A2 G6 G3 G7",
    "C1 F4 D1 W3",
    "E0 B2 F5 A4",
    "C2 A3 F6 D2",
    "B4 A6 C3+4 E2",
    "E1 A5 D4 F7",
    "B6 A7 C5+6 E4",
    "D6 D3 B7 C7",
    "E6 D5 D7 E3",
    "E5 E7",
)
f32 = jnp.float32
bf16 = jnp.bfloat16


def dot(a, b):
    return jnp.dot(a, b, preferred_element_type=f32)


def plain_schedule(n_ep, groups):
    words = ["H"] + [f"G{k}" for k in range(1, n_ep)] + ["O", "R"] + [f"F{n}" for n in range(8)]
    for t in range(groups + 4):
        for stage, lag in (("D", 3), ("E", 4), ("B", 1), ("C", 2), ("A", 0)):
            if 0 <= t - lag < groups:
                words.append(f"{stage}{t - lag}")
    return words


def kernel(
    n_ep,
    n_tp,
    capacity,
    value_hbm,
    gate_hbm,
    taps_hbm,
    bias_hbm,
    gain_hbm,
    shift_hbm,
    out_weight_hbm,
    out_bias_hbm,
    tokens_hbm,
    expert_gain_hbm,
    route_t_hbm,
    route_weight_t_hbm,
    gate_w_hbm,
    up_w_hbm,
    down_w_hbm,
    mixer,
    expert_out_ref,
    value,
    gate,
    taps_ref,
    bias_ref,
    gain_ref,
    shift_ref,
    out_weight,
    out_bias_ref,
    tokens_ref,
    expert_gain_ref,
    route_t_ref,
    route_weight_t_ref,
    gate_w,
    up_w,
    down_w,
    halo_out,
    halo_in,
    padded,
    filtered,
    activated,
    outgoing,
    outgoing_wide,
    arrived,
    hidden,
    partial,
    half_in,
    pair_out,
    pair_in,
    summed,
    returned,
    weight_high,
    weight_low,
    expert_sum,
    load_sem,
    halo_sem,
    disp_send,
    disp_recv,
    wide_send,
    wide_recv,
    f1_send,
    f1_recv,
    f2_send,
    f2_recv,
    r1_send,
    r1_recv,
    r2_send,
    r2_recv,
    ret_send,
    ret_recv,
):
    i = lax.axis_index("ep")
    q = lax.axis_index("tp")
    q1 = q + 1 - 2 * lax.rem(q, 2)
    q2 = lax.rem(q + 2, 4)
    q3 = lax.rem(q1 + 2, 4)
    tokens, width = tokens_ref.shape
    cols = width // n_tp
    rows_all = n_ep * capacity
    group_rows = max(128, capacity)
    per_group = group_rows // capacity
    groups = rows_all // group_rows
    length, channels = value.shape
    lane_tiles = channels // LANES
    taps = taps_ref.shape[0]
    rim = halo_out.shape[0]
    single = per_group == 1
    near = n_ep // 2 if single else 0
    here = i * n_tp + q
    last = n_ep * n_tp - 1
    following = lax.rem(here + 1, n_ep * n_tp)

    def peer(k):
        other, bit = 0, 1
        while bit < n_ep:
            other = other + bit * lax.rem(i // bit + k // bit, 2)
            bit *= 2
        return other

    barrier = pltpu.get_barrier_semaphore()

    def greet(ep, tp):
        pl.semaphore_signal(
            barrier,
            inc=1,
            device_id={"ep": ep, "tp": tp},
            device_id_type=pl.DeviceIdType.MESH,
        )

    def greet_peer(k, c):
        greet(peer(k), q)
        return c

    lax.fori_loop(1, n_ep, greet_peer, 0)
    greet(i, q1)
    greet(i, q2)

    @pl.when(here > 0)
    def _():
        greet((here - 1) // n_tp, lax.rem(here - 1, n_tp))

    copies = (
        ("route", route_t_hbm, route_t_ref),
        ("tokens", tokens_hbm, tokens_ref),
        ("expert_gain", expert_gain_hbm, expert_gain_ref),
        ("value", value_hbm, value),
        ("gate", gate_hbm, gate),
        ("taps", taps_hbm, taps_ref),
        ("bias", bias_hbm, bias_ref),
        ("gain", gain_hbm, gain_ref),
        ("shift", shift_hbm, shift_ref),
        ("out_bias", out_bias_hbm, out_bias_ref),
        ("weight_t", route_weight_t_hbm, route_weight_t_ref),
        ("gate_w", gate_w_hbm.at[0], gate_w),
        ("up_w", up_w_hbm.at[0], up_w),
        ("down_w", down_w_hbm.at[0], down_w),
        ("out_weight", out_weight_hbm, out_weight),
    )
    names = [name for name, _, _ in copies]
    loads = {
        name: pltpu.make_async_copy(s, d, load_sem.at[n])
        for n, (name, s, d) in enumerate(copies)
    }
    for name in names[:11]:
        loads[name].start()

    def remote(src, dst, send, recv, ep, tp):
        return pltpu.make_async_remote_copy(
            src_ref=src,
            dst_ref=dst,
            send_sem=send,
            recv_sem=recv,
            device_id={"ep": ep, "tp": tp},
            device_id_type=pl.DeviceIdType.MESH,
        )

    def block(k):
        return pl.ds(pl.multiple_of(k * capacity, capacity), capacity)

    def group(g):
        return pl.ds(g * group_rows, group_rows)

    def dispatch(k):
        return remote(
            outgoing.at[block(k)],
            arrived.at[q, block(k)],
            disp_send,
            disp_recv.at[k],
            peer(k),
            q,
        )

    def dispatch_wide(k):
        return remote(
            outgoing_wide.at[block(k)],
            arrived.at[q2, block(k)],
            wide_send,
            wide_recv.at[k - 1],
            peer(k),
            q,
        )

    def spread_pair(g):
        at = arrived.at[q, group(g)]
        return remote(at, at, f1_send, f1_recv.at[g - near], i, q2)

    def spread_core(g, n):
        at = arrived.at[q if n == 0 else q2, group(g)]
        return remote(at, at, f2_send, f2_recv.at[g], i, q1)

    def reduce_core(g, n):
        return remote(
            partial.at[q1 if n == 0 else q3, group(g)],
            half_in.at[n, group(g)],
            r1_send,
            r1_recv.at[g],
            i,
            q1,
        )

    def reduce_pair(g):
        return remote(
            pair_out.at[group(g)], pair_in.at[group(g)], r2_send, r2_recv.at[g], i, q2
        )

    def two_halves(send, recv, rows):
        at = half_in.at[:, pl.ds(0, rows)]
        return remote(at, at, send, recv, i, q1)

    def one_piece(send, rows):
        at = pair_in.at[pl.ds(0, rows)]
        return remote(at, at, send, r2_recv.at[0], i, q2)

    def give_back(k):
        return remote(
            summed.at[block(k)],
            returned.at[block(k)],
            ret_send,
            ret_recv.at[k],
            peer(k),
            q,
        )

    halo = remote(
        halo_out, halo_in, halo_sem.at[0], halo_sem.at[1], following // n_tp, lax.rem(following, n_tp)
    )

    def lower(a, b):
        return jnp.where(a < b, 1.0, 0.0).astype(bf16)

    side = (tokens, tokens)
    row_id = lax.broadcasted_iota(jnp.int32, side, 0)
    col_id = lax.broadcasted_iota(jnp.int32, side, 1)
    experts_t = lax.broadcasted_iota(jnp.int32, (n_ep, tokens), 0)
    loads["route"].wait()
    picks_t = [route_t_ref[n : n + 1, :] for n in range(route_t_ref.shape[0])]
    hot_t = [jnp.where(experts_t == p, 1.0, 0.0) for p in picks_t]
    rank_t = dot(sum(hot_t).astype(bf16), lower(row_id, col_id))
    slot_rows = lax.broadcasted_iota(jnp.int32, (rows_all, tokens), 0).astype(f32)
    chosen = jnp.zeros((rows_all, tokens), f32)
    targets = []
    for p, h in zip(picks_t, hot_t):
        target = (jnp.bitwise_xor(p, i) * capacity).astype(f32) + jnp.sum(
            rank_t * h, 0, keepdims=True
        )
        targets.append(target)
        chosen = jnp.where(slot_rows == target, 1.0, chosen)

    with jax.named_scope("w_tok"):
        loads["tokens"].wait()
    for name in names[11:]:
        loads[name].start()
    x = tokens_ref[...].astype(f32)
    scale = lax.rsqrt(jnp.mean(x * x, 1, keepdims=True) + epsilon)
    chosen = chosen.astype(bf16)
    loads["expert_gain"].wait()

    def columns(n):
        at = pl.ds(pl.multiple_of(n * cols, cols), cols)
        return (tokens_ref[:, at].astype(f32) * scale * expert_gain_ref[:, at]).astype(bf16)

    with jax.named_scope("select"):
        outgoing[...] = dot(chosen, columns(q)).astype(bf16)
        if near:
            outgoing_wide[...] = dot(chosen[0 : near * capacity], columns(q2)).astype(bf16)
    loads["value"].wait()
    loads["gate"].wait()
    edge = pl.ds(length - rim, rim)
    halo_out[...] = (value[edge].astype(f32) * jax.nn.sigmoid(gate[edge].astype(f32))).astype(bf16)

    with jax.named_scope("w_barrier"):
        pl.semaphore_wait(barrier, n_ep + 2 - jnp.where(here == last, 1, 0))

    @pl.when(here == 0)
    def _():
        halo_in[...] = jnp.zeros_like(halo_in)

    def start_halo():
        @pl.when(here < last)
        def _():
            halo.start()

    def send(k):
        dispatch(k).start()

    def send_wide(k):
        dispatch_wide(k).start()

    def own():
        with jax.named_scope("own"):
            if single:
                for n in range(n_tp):
                    arrived[n, 0:capacity] = dot(chosen[0:capacity], columns(n)).astype(bf16)
            else:
                arrived[q, 0:capacity] = outgoing[0:capacity]

    def gate_tile(l, c):
        at = pl.ds(pl.multiple_of(l * LANES, LANES), LANES)
        padded[l, rim:] = (
            (value[:, at].astype(f32) * jax.nn.sigmoid(gate[:, at].astype(f32)))
            .astype(bf16)
            .astype(f32)
        )
        return c

    def conv_tile(l, c):
        at = pl.ds(pl.multiple_of(l * LANES, LANES), LANES)
        padded[l, 0:rim] = halo_in[:, at].astype(f32)
        total = jnp.zeros((length, LANES), f32) + bias_ref[:, at]
        for j in range(taps):
            total = total + taps_ref[j : j + 1, at] * padded[l, pl.ds(rim - taps + 1 + j, length)]
        filtered[:, at] = total
        return c

    def norm_rows(r, c):
        at = pl.ds(pl.multiple_of(r * 32, 32), 32)
        f = filtered[at]
        centred = f - jnp.mean(f, 1, keepdims=True)
        variance = jnp.mean(centred * centred, 1, keepdims=True)
        v = centred * lax.rsqrt(variance + epsilon) * gain_ref[...] + shift_ref[...]
        activated[at] = (v * jax.nn.sigmoid(v)).astype(bf16)
        return c

    def project(n, c):
        at = pl.ds(pl.multiple_of(n * 256, 256), 256)
        mixer[:, at] = (dot(activated[...], out_weight[:, at]) + out_bias_ref[:, at]).astype(bf16)
        return c

    def experts_of(gs):
        ats = [group(g) for g in gs]
        held_rows = pl.ds(0, len(gs) * group_rows)

        def unit(n, c):
            u_at = pl.ds(pl.multiple_of(n * 256, 256), 256)
            rows = jnp.concatenate(
                [jnp.concatenate([arrived[s, at] for s in range(n_tp)], 1) for at in ats], 0
            )
            g_pre = dot(rows, gate_w[:, u_at])
            u_pre = dot(rows, up_w[:, u_at])
            held = jnp.minimum(g_pre, clamp_limit)
            up = jnp.clip(u_pre, -clamp_limit, clamp_limit)
            hidden[held_rows, u_at] = (held * jax.nn.sigmoid(swish_alpha * held) * (up + 1.0)).astype(bf16)
            return c

        lax.fori_loop(0, gate_w.shape[1] // 256, unit, 0)

        def down(s, c):
            at_cols = pl.ds(pl.multiple_of(s * cols, cols), cols)
            part = dot(hidden[held_rows, :], down_w[:, at_cols]).astype(bf16)
            for n, at in enumerate(ats):
                partial[s, at] = part[n * group_rows : (n + 1) * group_rows]
            return c

        lax.fori_loop(0, n_tp, down, 0)

    def arrive(k, c):
        dispatch(k).wait_recv()
        return c

    def give(k, c):
        give_back(k).start()
        return c

    if single and n_ep == 8:
        order = [0, 1, 4, 2, 5, 3, 6, 7]
    else:
        order = list(range(groups))
    wide = [g < near for g in order]

    def take(s):
        g = order[s]
        if single and s == 0:
            return
        with jax.named_scope(f"A{s}"):
            lax.fori_loop(jnp.maximum(g * per_group, 1), (g + 1) * per_group, arrive, 0)
            if wide[s]:
                dispatch_wide(g).wait_recv()
            else:
                spread_pair(g).start()
            spread_core(g, 0).start()
            if wide[s]:
                spread_core(g, 1).start()

    def relay(s):
        g = order[s]
        if wide[s]:
            return
        with jax.named_scope(f"B{s}"):
            spread_pair(g).wait_recv()
            spread_core(g, 1).start()

    def compute(*steps):
        for s in steps:
            if not (single and s == 0):
                with jax.named_scope(f"Cw{s}"):
                    two_halves(f2_send, f2_recv.at[order[s]], group_rows).wait_recv()
        with jax.named_scope(f"C{steps}"):
            experts_of([order[s] for s in steps])
        for s in steps:
            reduce_core(order[s], 0).start()
            reduce_core(order[s], 1).start()

    def halve(s):
        g = order[s]
        at = group(g)
        with jax.named_scope(f"D{s}"):
            two_halves(r1_send, r1_recv.at[g], group_rows).wait_recv()
            pair_out[at] = (partial[q2, at].astype(f32) + half_in[1, at].astype(f32)).astype(bf16)
            reduce_pair(g).start()

    def finish(s):
        g = order[s]
        at = group(g)
        with jax.named_scope(f"E{s}"):
            reduce_pair(g).wait_recv()
            summed[at] = (
                partial[q, at].astype(f32) + half_in[0, at].astype(f32) + pair_in[at].astype(f32)
            ).astype(bf16)
            lax.fori_loop(jnp.maximum(g * per_group, 1), (g + 1) * per_group, give, 0)

    def mixer_gate():
        lax.fori_loop(0, lane_tiles, gate_tile, 0)

    def mixer_halo():
        for name in ("taps", "bias", "gain", "shift"):
            loads[name].wait()

        @pl.when(here > 0)
        def _():
            halo.wait_recv()

    def mixer_conv(n):
        lax.fori_loop(n * lane_tiles // 2, (n + 1) * lane_tiles // 2, conv_tile, 0)

    def mixer_norm():
        lax.fori_loop(0, length // 32, norm_rows, 0)

    def mixer_project(n):
        if n == 0:
            loads["out_weight"].wait()
            loads["out_bias"].wait()
        tiles = out_weight.shape[1] // 256
        lax.fori_loop(n * tiles // 2, (n + 1) * tiles // 2, project, 0)

    def weigh():
        loads["weight_t"].wait()
        weights = jnp.zeros((rows_all, tokens), f32)
        for n, target in enumerate(targets):
            weights = jnp.where(slot_rows == target, route_weight_t_ref[n : n + 1, :], weights)
        weights = weights.T
        high = weights.astype(bf16)
        weight_high[...] = high
        weight_low[...] = (weights - high.astype(f32)).astype(bf16)

    fillers = [
        mixer_gate,
        mixer_halo,
        functools.partial(mixer_conv, 0),
        functools.partial(mixer_conv, 1),
        mixer_norm,
        functools.partial(mixer_project, 0),
        functools.partial(mixer_project, 1),
        weigh,
    ]

    def fill(n):
        with jax.named_scope(f"F{n}"):
            fillers[n]()

    def ready():
        for name in ("gate_w", "up_w", "down_w"):
            loads[name].wait()

    once = {"H": start_halo, "O": own, "R": ready}
    stages = {"A": take, "B": relay, "G": send, "W": send_wide, "C": compute, "D": halve, "E": finish, "F": fill}
    for word in " ".join(SCHEDULE).split() if single and n_ep == 8 else plain_schedule(n_ep, groups):
        if word in once:
            once[word]()
        else:
            stages[word[0]](*[int(n) for n in word[1:].split("+")])
    returned[0:capacity] = summed[0:capacity]

    def came_back(k, c):
        give_back(k).wait_recv()
        return c

    def weighted(low, high):
        at = pl.ds(low * capacity, (high - low) * capacity)
        return dot(weight_high[:, at], returned[at]) + dot(weight_low[:, at], returned[at])

    with jax.named_scope("w_ret"):
        if single:
            final = order[-1]
            lax.fori_loop(1, final, came_back, 0)
            expert_sum[...] = weighted(0, final)
            came_back(final, 0)
        else:
            lax.fori_loop(1, n_ep, came_back, 0)
    with jax.named_scope("final"):
        if single:
            expert_out_ref[...] = (expert_sum[...] + weighted(final, n_ep)).astype(bf16)
        else:
            expert_out_ref[...] = weighted(0, n_ep).astype(bf16)

    @pl.when(here < last)
    def _():
        halo.wait_send()

    lead = group_rows if single else 0
    with jax.named_scope("w_sent"):
        one_piece(disp_send, rows_all - capacity).wait_send()
        one_piece(ret_send, rows_all - capacity).wait_send()
        one_piece(r2_send, rows_all).wait_send()
        one_piece(f1_send, rows_all - near * group_rows).wait_send()
        two_halves(r1_send, r1_recv.at[0], rows_all).wait_send()
        two_halves(f2_send, f2_recv.at[0], rows_all - lead).wait_send()
        if near:
            one_piece(wide_send, (near - 1) * capacity).wait_send()


def publish(mixer, expert, mixer_hbm, expert_hbm, sems):
    copies = [
        pltpu.make_async_copy(mixer, mixer_hbm, sems.at[0]),
        pltpu.make_async_copy(expert, expert_hbm, sems.at[1]),
    ]
    for copy in copies:
        copy.start()
    for copy in copies:
        copy.wait()


def local(
    n_ep,
    n_tp,
    filter_value,
    filter_gate,
    filter_taps,
    filter_bias,
    norm_gain,
    norm_shift,
    out_weight,
    out_bias,
    expert_input,
    expert_gain,
    route_experts,
    route_weights,
    gate_weights,
    up_weights,
    down_weights,
):
    assert n_tp == 4 and n_ep & (n_ep - 1) == 0
    tokens, width = expert_input.shape
    capacity = 2 * tokens * route_experts.shape[1] // n_ep
    rows_all = n_ep * capacity
    group_rows = max(128, capacity)
    groups = rows_all // group_rows
    cols = width // n_tp
    length, channels = filter_value.shape
    units = gate_weights.shape[2]
    rim = -(-(filter_taps.shape[0] - 1) // 16) * 16
    vmem = pl.BlockSpec(memory_space=pltpu.VMEM)
    hbm = pl.BlockSpec(memory_space=pltpu.HBM)
    dma = pltpu.SemaphoreType.DMA
    operands = (
        filter_value,
        filter_gate,
        filter_taps,
        filter_bias[None],
        norm_gain[None],
        norm_shift[None],
        out_weight,
        out_bias[None],
        expert_input,
        expert_gain[None],
        route_experts.T,
        route_weights.T,
    )
    inputs = [
        pltpu.with_memory_space_constraint(a, pltpu.HBM)
        for a in operands + (gate_weights, up_weights, down_weights)
    ]
    results = (
        jax.ShapeDtypeStruct((length, out_weight.shape[1]), bf16),
        jax.ShapeDtypeStruct((tokens, cols), bf16),
    )
    mixed, expert_out = (
        pl.pallas_call(
            functools.partial(kernel, n_ep, n_tp, capacity),
            out_shape=results,
            in_specs=[hbm] * 15,
            out_specs=(vmem, vmem),
            scratch_shapes=[pltpu.VMEM(a.shape, a.dtype) for a in operands]
            + [
                pltpu.VMEM((width, units), bf16),
                pltpu.VMEM((width, units), bf16),
                pltpu.VMEM((units, width), bf16),
                pltpu.VMEM((rim, channels), bf16),
                pltpu.VMEM((rim, channels), bf16),
                pltpu.VMEM((channels // LANES, rim + length, LANES), f32),
                pltpu.VMEM((length, channels), f32),
                pltpu.VMEM((length, channels), bf16),
                pltpu.VMEM((rows_all, cols), bf16),
                pltpu.VMEM((rows_all // 2, cols), bf16),
                pltpu.VMEM((n_tp, rows_all, cols), bf16),
                pltpu.VMEM((2 * group_rows, units), bf16),
                pltpu.VMEM((n_tp, rows_all, cols), bf16),
                pltpu.VMEM((2, rows_all, cols), bf16),
                pltpu.VMEM((rows_all, cols), bf16),
                pltpu.VMEM((rows_all, cols), bf16),
                pltpu.VMEM((rows_all, cols), bf16),
                pltpu.VMEM((rows_all, cols), bf16),
                pltpu.VMEM((tokens, rows_all), bf16),
                pltpu.VMEM((tokens, rows_all), bf16),
                pltpu.VMEM((tokens, cols), f32),
                dma((15,)),
                dma((2,)),
                dma,
                dma((n_ep,)),
                dma,
                dma((n_ep // 2,)),
                dma,
                dma((groups,)),
                dma,
                dma((groups,)),
                dma,
                dma((groups,)),
                dma,
                dma((groups,)),
                dma,
                dma((n_ep,)),
            ],
            compiler_params=pltpu.CompilerParams(
                has_side_effects=True, collective_id=0, vmem_limit_bytes=44 * 1024 * 1024
            ),
            name="mixer_and_experts",
        )(*inputs)
    )
    return tuple(
        pl.pallas_call(
            publish,
            out_shape=results,
            in_specs=[vmem] * 2,
            out_specs=(hbm, hbm),
            scratch_shapes=[dma((2,))],
            compiler_params=pltpu.CompilerParams(vmem_limit_bytes=1024 * 1024),
            name="publish",
        )(mixed, expert_out)
    )


def solution(mesh):
    in_specs = (
        P(("ep", "tp"), None),
        P(("ep", "tp"), None),
        P(),
        P(),
        P(),
        P(),
        P(),
        P(),
        P("ep", None),
        P(),
        P("ep", None),
        P("ep", None),
        P("ep", None, "tp"),
        P("ep", None, "tp"),
        P("ep", "tp", None),
    )
    out_specs = (P(("ep", "tp"), None), P("ep", "tp"))
    body = functools.partial(local, mesh.shape["ep"], mesh.shape["tp"])
    return jax.shard_map(body, mesh=mesh, in_specs=in_specs, out_specs=out_specs, check_vma=False)
```
